32 devices in a mesh: grp: 2 (over y), fs: 4 (over z), tp: 4 (over x, core).
Axes of the slice: x: 2, y: 2, z: 4, core: 2. Of those that a mesh axis runs over, the one named last changes fastest.
Arguments:
- tokens: bfloat16 [1536, 2048], P(('grp', 'tp')), parts along dimension 0, may hold values from -6 to 6
- routes: int32 [1536, 2], P(('grp', 'tp')), parts along dimension 0, may hold values from 0 to 3, all different within a row; in each aligned block of 192 rows (0 to 191, 192 to 383, ...) at most 128 rows name the same one
- route_weight: float32 [1536, 2], P(('grp', 'tp')), parts along dimension 0, may hold values from 0.2 to 1
- norm_gain: float32 [2048], P('fs'), may hold values from 0.1 to 1.9
- gate_train: float32 [4, 2048, 5632], P('tp', 'fs'), may hold values from -0.125 to 0.125
- up_train: float32 [4, 2048, 5632], P('tp', 'fs'), may hold values from -0.125 to 0.125
- down_train: float32 [4, 5632, 2048], P('tp', None, 'fs'), may hold values from -0.109375 to 0.109375
Outputs:
- gate_serve: bfloat16 [8, 2048, 5632], P(('grp', 'tp'), None, 'fs'), parts along dimension 0
- up_serve: bfloat16 [8, 2048, 5632], P(('grp', 'tp'), None, 'fs'), parts along dimension 0
- down_serve: bfloat16 [8, 5632, 2048], P(('grp', 'tp'), 'fs'), parts along dimension 0
- mixed: bfloat16 [1536, 2048], P(('grp', 'tp'), 'fs'), parts along dimension 0
The draws below stay inside these ranges and needn't reach their ends.
There are 2 independent parts, one for each index of `grp`. The reference program is written for one: setup_inputs(seed, part) draws one part's arguments, and reference() takes and returns one part's arrays. A program takes and returns all parts, laid end to end along the dimension named above; an argument that names none is the same for every part. Nothing has to cross between parts.
Inputs may be any that keep to these rules, and one draw needn't show every extreme that they name: `routes`: each row names 2 different experts. In each aligned block of 192 rows no expert is named by more than 128 rows, a bound that some block reaches.
All inputs are finite; a program needn't handle non-finite values.
Results may differ from the reference program's by a relative error of at most 0.0087.
Values may be sent and summed in bfloat16 or wider, within the bound.
A program may use at most 128 MiB of HBM per device.

```python
import math
import jax
import jax.numpy as jnp
import numpy as np
from jax import lax

D = 2048
FF = 5632
EXPERTS = 4
TOP = 2
TOK_DEV = 192
CAP = 128
TOKENS = 768
COPIES = 1


def strengthened(values, own_key, source, target, blocks, factor):
    def block_of(axis_at):
        return (jnp.arange(values.shape[axis_at]) // (values.shape[axis_at] // blocks)).reshape((-1,) + (1,) * (values.ndim - 1 - axis_at))

    one_side = jax.random.permutation(own_key, blocks)[block_of(target)]
    other_side = (block_of(target) + blocks // 2) % blocks
    return jnp.where((block_of(source) == one_side) | (block_of(source) == other_side), factor * values, values)


def levels(key, extent, pieces, least, largest):
    loudness = 1.0
    for dim, blocks in pieces:
        draws = jax.random.uniform(jax.random.fold_in(jax.random.fold_in(key, 6), dim), (blocks,), jnp.float32, least / len(pieces), largest / len(pieces))
        loudness = loudness * jnp.repeat(jnp.exp(draws), extent[dim] // blocks).reshape((-1,) + (1,) * (len(extent) - 1 - dim))
    return loudness


def routed_block(own_key, own, number, rows, count, top, bound, lean):
    order = jax.random.permutation(own_key, count)
    packed, usual = portions_of(count, rows * top, bound, lean, True), portions_of(count, rows * top, bound, lean, False)
    places = jnp.arange(count)

    def named(lengths, turn):
        used = int((lengths > 0).sum())
        fixed = max(1, used // 4)
        moved = fixed + (places - fixed + turn * (used - fixed)) % max(1, count - fixed)
        return jnp.zeros((count,), jnp.int32).at[order[jnp.where(places < fixed, places, moved)]].set(jnp.asarray(lengths, jnp.int32))

    lengths = jnp.where(number % 4 == 0, named(packed, number // 4), named(usual, number - number // 4 - 1))
    mixed = jax.random.permutation(jax.random.fold_in(own, 3), count)
    giver, sink = mixed[0:count // 2 * 2:2], mixed[1:count // 2 * 2:2]
    slack = jnp.minimum(lengths[giver] - 1, bound - lengths[sink]) // 2
    slack = jnp.where((giver == order[0]) | (sink == order[0]) | (lengths[sink] == 0), 0, jnp.maximum(slack, 0))
    moved = jax.random.randint(jax.random.fold_in(own, 4), (count // 2,), 0, 1 << 20) % (slack + 1)
    lengths = lengths.at[giver].add(-moved).at[sink].add(moved)
    items = jnp.searchsorted(jnp.cumsum(lengths), jnp.arange(rows * top), side="right").astype(jnp.int32)
    table = items.reshape(top, rows).T
    table = table[jax.random.permutation(jax.random.fold_in(own, 1), rows)]
    turn = jax.random.randint(jax.random.fold_in(own, 2), (rows, 1), 0, top)
    return jnp.take_along_axis(table, (jnp.arange(top)[None, :] + turn) % top, axis=1)


def portions_of(amount, total, limit, slope, full):
    weights = [(1 << 20) // math.isqrt(grade ** slope) + 1 for grade in range(1, amount + 1)]
    largest = limit if full else min(limit, max(-(-total // amount), total * weights[0] // sum(weights)))
    least = 1 if total - largest >= amount - 1 else 0
    holding, rest = [largest] + [least] * (amount - 1), total - largest - least * (amount - 1)
    while rest > 0:
        movable = [i for i in range(1, amount) if holding[i] < largest] or [i for i in range(1, amount) if holding[i] < limit]
        whole, left = sum([weights[i] for i in movable]), rest
        for i in movable:
            extra = min(limit - holding[i], max(1, left * weights[i] // whole), rest)
            holding[i] = holding[i] + extra
            rest = rest - extra
    return np.array(holding)


def gaussian(key, shape, width, limit, pieces=(), kind=jnp.bfloat16):
    values = jax.random.normal(key, shape, jnp.float32) * width
    if len(pieces) > 0:
        values = levels(key, shape, pieces, -0.22, 0.18) * values
    return jnp.clip(values, min=-limit, max=limit).astype(kind)


def gaussian_with(stream_key, dims, spread, most, split, heavy, held_as=jnp.bfloat16):
    drawn = spread * jax.random.normal(stream_key, dims, jnp.float32)
    if split:
        drawn = drawn * levels(stream_key, dims, split, -0.22, 0.18)
    return jnp.clip(strengthened(drawn, jax.random.fold_in(stream_key, 3), *heavy), -most, most).astype(held_as)


def setup_inputs(seed: int = 0, part: int = 0) -> dict:
    streams_of = jax.random.split(jax.random.key(seed), 8)
    part_splits = jax.random.split(jax.random.fold_in(streams_of[7], part), 8)
    tokens = gaussian(part_splits[0], (TOKENS, D), 1.0, 6.0, ((0, 4),))
    routes_keys = jax.random.split(jax.random.fold_in(part_splits[1], 1), TOKENS // TOK_DEV)
    routes_turns = jax.random.permutation(jax.random.fold_in(part_splits[1], 3), TOKENS // TOK_DEV)
    routes = jax.vmap(lambda own, number: routed_block(jax.random.fold_in(part_splits[1], 2), own, number, TOK_DEV, EXPERTS, TOP, CAP, 1))(routes_keys, routes_turns).reshape((TOKENS, TOP))
    route_weight = jnp.clip(0.2 + 0.8 * jax.random.uniform(part_splits[2], (TOKENS, TOP), jnp.float32) ** levels(part_splits[2], (TOKENS, TOP), ((0, 4),), -0.2, 0.2), 0.2, 1.0)
    norm_gain = jnp.clip(1.0 + 0.18 * jax.random.normal(streams_of[3], (D,), jnp.float32), 0.1, 1.9)
    gate_train = gaussian(streams_of[4], (EXPERTS, D, FF), D ** -0.5, 0.125, ((0, 4), (1, 4)), jnp.float32)
    up_train = gaussian(streams_of[5], (EXPERTS, D, FF), D ** -0.5, 0.125, ((0, 4), (1, 4)), jnp.float32)
    down_train = gaussian_with(streams_of[6], (EXPERTS, FF, D), FF ** -0.5, 0.109375, ((0, 4), (2, 4)), (1, 2, 4, 2.0), jnp.float32)
    return {"tokens": tokens, "routes": routes, "route_weight": route_weight, "norm_gain": norm_gain, "gate_train": gate_train, "up_train": up_train, "down_train": down_train}


def reference(tokens, routes, route_weight, norm_gain, gate_train, up_train, down_train):
    gain_column = norm_gain[None, :, None]
    gate_low = (gate_train * gain_column).astype(jnp.bfloat16)
    up_low = (up_train * gain_column).astype(jnp.bfloat16)
    down_low = down_train.astype(jnp.bfloat16)
    tok_float = tokens.astype(jnp.float32)
    normed = (tok_float * lax.rsqrt(lax.optimization_barrier(jnp.mean(tok_float * tok_float, axis=-1, keepdims=True)) + 1e-06)).astype(jnp.bfloat16)
    normed_wide = normed.astype(jnp.float32)

    def expert(triple):
        gate_one, up_one, down_one = triple
        gated = jnp.dot(normed_wide, gate_one.astype(jnp.float32), preferred_element_type=jnp.float32)
        lifted = jnp.dot(normed_wide, up_one.astype(jnp.float32), preferred_element_type=jnp.float32)
        hidden = (jax.nn.silu(gated) * lifted).astype(jnp.bfloat16)
        return jnp.dot(hidden.astype(jnp.float32), down_one.astype(jnp.float32), preferred_element_type=jnp.float32).astype(jnp.bfloat16)
    outputs = lax.map(expert, (gate_low, up_low, down_low))
    row_index = jnp.arange(tokens.shape[0], dtype=jnp.int32)
    first = outputs[routes[:, 0], row_index].astype(jnp.float32)
    second = outputs[routes[:, 1], row_index].astype(jnp.float32)
    mixed = route_weight[:, 0:1] * first + route_weight[:, 1:2] * second
    gate_serve = jnp.tile(gate_low, (1, 1, COPIES))
    up_serve = jnp.tile(up_low, (1, 1, COPIES))
    down_serve = jnp.tile(down_low, (1, COPIES, 1))
    return (gate_serve, up_serve, down_serve, mixed.astype(jnp.bfloat16))
```

```python
import functools
import jax
import jax.numpy as jnp
from jax import lax
from jax.experimental import pallas as pl
from jax.experimental.pallas import tpu as pltpu
from jax.sharding import PartitionSpec as P

EXPERTS = 4
CAP = 128
MESH = pl.DeviceIdType.MESH


def exchange_kernel(F, T, R, C, Q, gt, ut, dt, gain, tokens, routes_t, weight_t, gw, uw, dw, mown, mrecv,
                    flat, turned, scale_at, wide, tall, sendw, sendt, normed, xs, bh, bl,
                    arr, gacc, uacc, hid, pbf, ret, msend, shared,
                    zs, zr, ys, yr, ts, tr, ps, pr, ms, mr, loc):
    g, f, t = lax.axis_index("grp"), lax.axis_index("fs"), lax.axis_index("tp")
    H = R // 2
    wins = (gw, uw, dw)
    low = 1 - lax.div(f, 2)
    inner = lax.rem(lax.div(f + 1, 2), 2)
    near = f + 1 - 2 * lax.rem(f, 2)
    far_in = 1 + low
    far_out = 3 * low
    peers = [lax.rem(t + d, T) for d in range(1, T)]
    others = [near, far_in, far_out]

    def pick(if_inner, if_outer):
        return inner * if_inner + (1 - inner) * if_outer

    cross = pick(far_in, far_out)
    targets = (
        (pick(far_out, near), pick(near, far_in), pick(far_in, far_out)),
        (near, far_in, far_out),
        (near, pick(far_out, far_in), pick(far_in, far_out)),
    )
    sources = (
        (pick(near, far_in), pick(far_out, near), pick(far_in, far_out)),
        (near, far_out, far_in),
        (near, far_out, far_in),
    )

    barrier = pltpu.get_barrier_semaphore()
    for p in peers:
        pl.semaphore_signal(barrier, inc=1, device_id={"tp": p}, device_id_type=MESH)
    for p in others:
        pl.semaphore_signal(barrier, inc=1, device_id={"fs": p}, device_id_type=MESH)
    pl.semaphore_signal(barrier, inc=1, device_id={"grp": 1 - g}, device_id_type=MESH)

    def cols_of(src, half):
        return pl.ds(pl.multiple_of(src * R + half * H, H), H)

    def half_cols(half):
        return pl.ds(pl.multiple_of(half * H, H), H)

    def part(a, src, half, q):
        if a < 2:
            return wins[a].at[pl.ds(pl.multiple_of(src * R + half * H + q * (H // Q), H // Q), H // Q), :]
        return dw.at[pl.ds(q * (C // Q), C // Q), cols_of(src, half)]

    def z_copy(a, k, q):
        piece = sendw.at[a, k, pl.ds(q * (H // Q), H // Q), :] if a < 2 else sendt.at[k, pl.ds(q * (C // Q), C // Q), :]
        return pltpu.make_async_remote_copy(
            src_ref=piece, dst_ref=part(a, f, g, q), send_sem=zs.at[a, k, q], recv_sem=zr.at[a, f, q],
            device_id={"fs": targets[a][k]}, device_id_type=MESH)

    def z_send(a, k):
        for q in range(Q):
            z_copy(a, k, q).start()

    def z_recv(a, src, q):
        return pltpu.make_async_remote_copy(
            src_ref=part(a, src, g, q), dst_ref=part(a, src, g, q), send_sem=zs.at[a, 0, q],
            recv_sem=zr.at[a, src, q], device_id={"fs": src}, device_id_type=MESH)

    def y_copy(a, src, half, q):
        return pltpu.make_async_remote_copy(
            src_ref=part(a, src, half, q), dst_ref=part(a, src, half, q), send_sem=ys.at[a, src, q],
            recv_sem=yr.at[a, src, q], device_id={"grp": 1 - g}, device_id_type=MESH)

    def slots(q):
        return pl.ds(pl.multiple_of(q * CAP, CAP), CAP)

    def t_copy(tgt, src):
        return pltpu.make_async_remote_copy(
            src_ref=xs.at[slots(tgt), :], dst_ref=arr.at[slots(src), :], send_sem=ts.at[tgt], recv_sem=tr.at[src],
            device_id={"tp": tgt}, device_id_type=MESH)

    def p_copy(c, half, tgt, src):
        cols = cols_of(c, half)
        return pltpu.make_async_remote_copy(
            src_ref=pbf.at[slots(tgt), cols], dst_ref=ret.at[slots(src), cols],
            send_sem=ps.at[c, half, tgt], recv_sem=pr.at[c, half, src],
            device_id={"tp": tgt}, device_id_type=MESH)

    def m_copy(kind, block, half):
        dst = shared.at[:, half_cols(half)] if kind == 2 else mrecv.at[kind, :, half_cols(half)]
        return pltpu.make_async_remote_copy(
            src_ref=msend.at[:, cols_of(block, half)], dst_ref=dst,
            send_sem=ms.at[kind, half], recv_sem=mr.at[kind, half],
            device_id={"fs": cross if kind == 1 else near}, device_id_type=MESH)

    tasks = [(a, k, g) for a in range(3) for k in range(3)]
    tasks += [(a, None, half) for a in range(3) for half in range(2)]

    def stage_copy(n):
        a, k, half = tasks[n]
        tgt = f if k is None else targets[a][k]
        rows, cols = half_cols(half), pl.ds(pl.multiple_of(tgt * C, C), C)
        if a < 2:
            return pltpu.make_async_copy((gt, ut)[a].at[rows, cols], wide.at[n % 3], loc.at[n % 3])
        return pltpu.make_async_copy(dt.at[cols, rows], tall.at[n % 3], loc.at[3 + n % 3])

    def cast_wide(n, begin, end):
        a, k, half = tasks[n]

        @pl.loop(begin // 32, end // 32)
        def _(m):
            rows = pl.ds(pl.multiple_of(m * 32, 32), 32)
            scale = scale_at[pl.ds(pl.multiple_of(half * H + m * 32, 32), 32), 0:1]
            value = (wide[n % 3, rows, :] * scale).astype(jnp.bfloat16)
            if k is None:
                wins[a][pl.ds(pl.multiple_of(f * R + half * H + m * 32, 32), 32), :] = value
            else:
                sendw[a, k, rows, :] = value

    def cast(n):
        a, k, half = tasks[n]
        stage_copy(n).wait()
        if a < 2:
            cast_wide(n, 0, H)
        else:
            @pl.loop(0, C // 128)
            def _(m):
                rows = pl.ds(pl.multiple_of(m * 128, 128), 128)
                value = tall[n % 3, rows, :].astype(jnp.bfloat16)
                if k is None:
                    dw[rows, cols_of(f, half)] = value
                else:
                    sendt[k, rows, :] = value
        if n + 3 < len(tasks):
            stage_copy(n + 3).start()

    def route():
        tok, slot_all = tokens.shape[0], arr.shape[0]

        @pl.loop(0, tok // 32)
        def _(m):
            rows = pl.ds(pl.multiple_of(m * 32, 32), 32)
            value = tokens[rows, :].astype(jnp.float32)
            normed[rows, :] = (
                value * lax.rsqrt(jnp.mean(value * value, axis=-1, keepdims=True) + 1e-06)
            ).astype(jnp.bfloat16)

        one, two = routes_t[0:1, :], routes_t[1:2, :]
        row = lax.broadcasted_iota(jnp.int32, (tok, tok), 0)
        col = lax.broadcasted_iota(jnp.int32, (tok, tok), 1)
        expert = lax.broadcasted_iota(jnp.int32, (16, tok), 0)
        hot = jnp.where((expert == one) | (expert == two), 1.0, 0.0).astype(jnp.bfloat16)
        before = jnp.dot(hot, jnp.where(row < col, 1.0, 0.0).astype(jnp.bfloat16), preferred_element_type=jnp.float32)
        first, second = [
            name.astype(jnp.float32) * CAP
            + jnp.sum(jnp.where(expert == name, before, 0.0), axis=0, keepdims=True)
            for name in (one, two)
        ]
        slot = lax.broadcasted_iota(jnp.int32, (slot_all, tok), 0).astype(jnp.float32)
        select = jnp.where((slot == first) | (slot == second), 1.0, 0.0).astype(jnp.bfloat16)
        for n in range(4):
            cols = pl.ds(n * (F * R // 4), F * R // 4)
            xs[:, cols] = jnp.dot(select, normed[:, cols], preferred_element_type=jnp.float32).astype(jnp.bfloat16)
        flat[...] = jnp.zeros_like(flat)
        for n, line in enumerate((first, second, weight_t[0:1, :], weight_t[1:2, :])):
            flat[n:n + 1, 0:tok] = line
        turned[...] = flat[...].T
        slot = lax.broadcasted_iota(jnp.int32, (tok, slot_all), 1).astype(jnp.float32)
        blend = jnp.where(slot == turned[0:tok, 0:1], turned[0:tok, 2:3], 0.0) + jnp.where(
            slot == turned[0:tok, 1:2], turned[0:tok, 3:4], 0.0)
        high = blend.astype(jnp.bfloat16)
        bh[...] = high
        bl[...] = (blend - high.astype(jnp.float32)).astype(jnp.bfloat16)

    for n in range(3):
        stage_copy(n).start()
    for n in range(R // 128):
        piece = pl.ds(n * 128, 128)
        scale_at[piece, :] = jnp.broadcast_to(gain[0:1, piece], (128, 128)).T
    stage_copy(0).wait()
    for q in range(Q):
        cast_wide(0, q * (H // Q), (q + 1) * (H // Q))
        if q == 0:
            pl.semaphore_wait(barrier, len(peers) + len(others) + 1)
        else:
            z_copy(0, 0, q - 1).start()
    stage_copy(3).start()
    for n in range(1, 9):
        cast(n)
        a, k = tasks[n - 1][:2]
        if n == 1:
            z_copy(0, 0, Q - 1).start()
        elif a == 2 and k > 0:
            @pl.when(inner == 1)
            def _():
                z_send(a, k)
        else:
            z_send(a, k)
    route()

    @pl.when(inner == 1)
    def _():
        z_send(2, 2)

    for n in range(9, len(tasks)):
        cast(n)
        if n == 9:
            for p in peers:
                t_copy(p, t).start()
    arr[slots(t), :] = xs[slots(t), :]

    rows_all = arr.shape[0]
    M = min(256, rows_all)

    def multiply(a, src, first):
        acc = (gacc, uacc)[a]
        deep = pl.ds(pl.multiple_of(src * R, R), R)

        @pl.loop(0, rows_all // M)
        def _(m):
            rows = pl.ds(pl.multiple_of(m * M, M), M)
            value = jnp.dot(arr[rows, deep], wins[a][deep, :], preferred_element_type=jnp.float32)
            if first:
                acc[rows, :] = value
            else:
                acc[rows, :] += value

    def activate():
        @pl.loop(0, rows_all // 64)
        def _(m):
            rows = pl.ds(pl.multiple_of(m * 64, 64), 64)
            v = gacc[rows, :]
            hid[rows, :] = (v / (1.0 + jnp.exp(-v)) * uacc[rows, :]).astype(jnp.bfloat16)

    def partial_out(src, half):
        cols = cols_of(src, half)

        @pl.loop(0, rows_all // M)
        def _(m):
            rows = pl.ds(pl.multiple_of(m * M, M), M)
            pbf[rows, cols] = jnp.dot(hid[rows, :], dw[:, cols], preferred_element_type=jnp.float32).astype(jnp.bfloat16)

        for p in peers:
            p_copy(src, half, p, t).start()
        ret[slots(t), cols] = pbf[slots(t), cols]

    def mix(src, half):
        cols = cols_of(src, half)
        for p in peers:
            p_copy(src, half, p, p).wait_recv()
        return jnp.dot(bh[...], ret[:, cols], preferred_element_type=jnp.float32) + jnp.dot(
            bl[...], ret[:, cols], preferred_element_type=jnp.float32)

    def mix_own(half):
        mown[:, half_cols(half)] = mix(f, half)

    def mix_near(half):
        msend[:, cols_of(near, half)] = mix(near, half).astype(jnp.bfloat16)
        m_copy(0, near, half).start()

    def mix_far(src, half, joins):
        cols = cols_of(src, half)
        value = mix(src, half)

        @pl.when(joins == 1)
        def _():
            m_copy(2, src, half).wait_recv()
            both = value + shared[:, half_cols(half)].astype(jnp.float32)
            msend[:, cols] = both.astype(jnp.bfloat16)
            m_copy(1, src, half).start()

        @pl.when(joins == 0)
        def _():
            msend[:, cols] = value.astype(jnp.bfloat16)
            m_copy(2, src, half).start()

    def arrive(a, src, middle=None):
        for q in range(Q):
            z_recv(a, src, q).wait_recv()
            y_copy(a, src, g, q).start()
            if q == 1 and middle is not None:
                middle()

    def settle(a, src):
        for q in range(Q):
            y_copy(a, src, 1 - g, q).wait_recv()
        if a < 2:
            multiply(a, src, False)

    items = [(a, sources[a][k]) for a in range(2) for k in range(3)]
    arrive(*items[0])
    arrive(*items[1])
    for p in peers:
        t_copy(p, p).wait_recv()
    for a in (0, 1):
        multiply(a, f, True)
    settle(*items[0])
    for n in range(2, 6):
        arrive(*items[n], middle=functools.partial(settle, *items[n - 1]))

    @pl.when(inner == 0)
    def _():
        z_send(2, 1)
        z_send(2, 2)

    arrive(2, near)
    settle(*items[5])
    activate()
    partial_out(f, 0)
    partial_out(f, 1)
    partial_out(near, g)
    settle(2, near)
    partial_out(near, 1 - g)
    mix_own(0)
    mix_own(1)
    mix_near(g)
    arrive(2, far_out, middle=functools.partial(mix_near, 1 - g))
    partial_out(far_out, g)
    settle(2, far_out)
    partial_out(far_out, 1 - g)
    mix_far(far_out, g, 1 - inner)
    mix_far(far_out, 1 - g, 1 - inner)
    arrive(2, far_in)
    partial_out(far_in, g)
    settle(2, far_in)
    partial_out(far_in, 1 - g)
    mix_far(far_in, g, inner)
    mix_far(far_in, 1 - g, inner)
    for half in range(2):
        for kind in range(2):
            m_copy(kind, near, half).wait_recv()

    for p in peers:
        t_copy(p, t).wait_send()
        for c in range(F):
            for half in range(2):
                p_copy(c, half, p, t).wait_send()
    for a in range(3):
        for k in range(3):
            for q in range(Q):
                z_copy(a, k, q).wait_send()
                y_copy(a, others[k], g, q).wait_send()
    for half in range(2):
        for kind in range(3):
            m_copy(kind, near, half).wait_send()


def deliver_kernel(gw, uw, dw, mown, mrecv, go, uo, do, mo, total, sems):
    copies = [pltpu.make_async_copy(a, b, sems.at[n]) for n, (a, b) in enumerate(((gw, go), (uw, uo), (dw, do)))]
    for copy in copies:
        copy.start()
    value = mown[...]
    for n in range(mrecv.shape[0]):
        value = value + mrecv[n].astype(jnp.float32)
    total[...] = value.astype(jnp.bfloat16)
    last = pltpu.make_async_copy(total, mo, sems.at[len(copies)])
    last.start()
    for copy in copies + [last]:
        copy.wait()


def exchange(F, T, gate, up, down, gain, tokens, routes, weight):
    span = -(-tokens.shape[0] // 128) * 128
    R, FF = gate.shape
    C, D, H = FF // F, F * R, R // 2
    Q = 4
    tok, S = tokens.shape[0], EXPERTS * CAP
    bf, f32 = jnp.bfloat16, jnp.float32
    any_spec, vm = pl.BlockSpec(memory_space=pl.ANY), pl.BlockSpec(memory_space=pltpu.VMEM)
    dma = pltpu.SemaphoreType.DMA
    held = pl.pallas_call(
        functools.partial(exchange_kernel, F, T, R, C, Q),
        name="exchange",
        out_shape=(pltpu.VMEM((D, C), bf), pltpu.VMEM((D, C), bf), pltpu.VMEM((C, D), bf),
                   pltpu.VMEM((tok, R), f32), pltpu.VMEM((2, tok, R), bf)),
        in_specs=[any_spec] * 3 + [vm] * 4,
        out_specs=(vm,) * 5,
        scratch_shapes=[
            pltpu.VMEM((128, span), f32), pltpu.VMEM((span, 128), f32), pltpu.VMEM((R, 128), f32),
            pltpu.VMEM((3, H, C), f32), pltpu.VMEM((3, C, H), f32),
            pltpu.VMEM((2, F - 1, H, C), bf), pltpu.VMEM((F - 1, C, H), bf),
            pltpu.VMEM((tok, D), bf), pltpu.VMEM((S, D), bf), pltpu.VMEM((tok, S), bf), pltpu.VMEM((tok, S), bf),
            pltpu.VMEM((S, D), bf),
            pltpu.VMEM((S, C), f32), pltpu.VMEM((S, C), f32), pltpu.VMEM((S, C), bf),
            pltpu.VMEM((S, D), bf), pltpu.VMEM((S, D), bf), pltpu.VMEM((tok, D), bf), pltpu.VMEM((tok, R), bf),
            dma((3, F - 1, Q)), dma((3, F, Q)), dma((3, F, Q)), dma((3, F, Q)), dma((T,)), dma((T,)),
            dma((F, 2, T)), dma((F, 2, T)), dma((3, 2)), dma((3, 2)), dma((6,)),
        ],
        compiler_params=pltpu.CompilerParams(collective_id=0, has_side_effects=True, vmem_limit_bytes=42 * 1024 * 1024),
    )(gate, up, down, gain[None, :], tokens, routes.T, weight.T)
    return pl.pallas_call(
        deliver_kernel,
        name="deliver",
        out_shape=(jax.ShapeDtypeStruct((D, C), bf), jax.ShapeDtypeStruct((D, C), bf),
                   jax.ShapeDtypeStruct((C, D), bf), jax.ShapeDtypeStruct((tok, R), bf)),
        in_specs=[vm] * 5,
        out_specs=(pl.BlockSpec(memory_space=pltpu.HBM),) * 4,
        scratch_shapes=[pltpu.VMEM((tok, R), bf), dma((4,))],
        compiler_params=pltpu.CompilerParams(vmem_limit_bytes=4 * 1024 * 1024),
    )(*[pltpu.with_memory_space_constraint(x, pltpu.VMEM) for x in held])


def fits(grp_count, fs_count, pieces, gate_train):
    rows, wide = gate_train.shape[1:]
    return (grp_count == 2 and fs_count == pieces and fs_count == 4
            and wide % (fs_count * 128) == 0 and rows % 256 == 0)


def shards(tokens, routes, route_weight, norm_gain, gate_train, up_train, down_train):
    fs_count = lax.axis_size("fs")
    pieces = min(fs_count, 32)
    copies = fs_count // pieces
    if fits(lax.axis_size("grp"), fs_count, pieces, gate_train):
        gate_new, up_new, down_new, mixed = exchange(
            fs_count, lax.axis_size("tp"), gate_train[0], up_train[0], down_train[0],
            norm_gain, tokens, routes, route_weight,
        )
        return (gate_new[None], up_new[None], down_new[None], mixed)
    gain_column = norm_gain[:, None]
    gate_low = (gate_train[0] * gain_column).astype(jnp.bfloat16)
    up_low = (up_train[0] * gain_column).astype(jnp.bfloat16)
    down_low = down_train[0].astype(jnp.bfloat16)
    gate_wide = jnp.tile(gate_low, (1, copies))
    up_wide = jnp.tile(up_low, (1, copies))
    down_wide = jnp.tile(down_low, (copies, 1))
    gate_new, up_new = (
        lax.all_to_all(gate_wide, "fs", split_axis=1, concat_axis=0, tiled=True),
        lax.all_to_all(up_wide, "fs", split_axis=1, concat_axis=0, tiled=True),
    )
    down_new = lax.all_to_all(down_wide, "fs", split_axis=0, concat_axis=1, tiled=True)
    tok_float = tokens.astype(jnp.float32)
    normed = (
        tok_float * lax.rsqrt(jnp.mean(tok_float * tok_float, axis=-1, keepdims=True) + 1e-06)
    ).astype(jnp.bfloat16)
    chosen = routes.reshape(-1)
    chosen_hot = (chosen[:, None] == jnp.arange(EXPERTS, dtype=jnp.int32)[None, :]).astype(
        jnp.int32
    )
    before = jnp.cumsum(chosen_hot, axis=0) - chosen_hot
    slot_rank = jnp.sum(before * chosen_hot, axis=1)
    slot_index = (chosen * CAP + slot_rank).reshape(routes.shape)
    slot_range = jnp.arange(EXPERTS * CAP, dtype=jnp.int32)
    select_rows = jnp.any(slot_range[:, None, None] == slot_index[None, :, :], axis=-1).astype(
        jnp.bfloat16
    )
    outgoing = jnp.dot(select_rows, normed, preferred_element_type=jnp.float32).astype(jnp.bfloat16)
    outgoing = outgoing.reshape(EXPERTS, CAP, normed.shape[1])
    arrived = lax.all_to_all(outgoing, "tp", split_axis=0, concat_axis=0, tiled=True).reshape(
        EXPERTS * CAP, normed.shape[1]
    )
    slot_count = EXPERTS * CAP // copies
    copy_index = lax.axis_index("fs") // pieces
    my_rows = lax.dynamic_slice_in_dim(arrived, copy_index * slot_count, slot_count, 0)
    gated = jnp.dot(my_rows, gate_new, preferred_element_type=jnp.float32)
    lifted = jnp.dot(my_rows, up_new, preferred_element_type=jnp.float32)
    hidden = (jax.nn.silu(gated) * lifted).astype(jnp.bfloat16)
    partial_out = jnp.dot(hidden, down_new, preferred_element_type=jnp.float32)
    placed = jnp.zeros((EXPERTS * CAP, partial_out.shape[1]), jnp.float32)
    placed = lax.dynamic_update_slice_in_dim(placed, partial_out, copy_index * slot_count, 0)
    expert_out = lax.psum_scatter(placed, "fs", scatter_dimension=1, tiled=True).astype(
        jnp.bfloat16
    )
    returned = lax.all_to_all(
        expert_out.reshape(EXPERTS, CAP, expert_out.shape[1]),
        "tp",
        split_axis=0,
        concat_axis=0,
        tiled=True,
    )
    returned = returned.reshape(EXPERTS * CAP, expert_out.shape[1]).astype(jnp.float32)
    blend_weight = jnp.sum(
        jnp.where(
            slot_range[None, None, :] == slot_index[:, :, None], route_weight[:, :, None], 0.0
        ),
        axis=1,
    )
    mixed = jnp.dot(
        blend_weight, returned, precision=lax.Precision.HIGHEST, preferred_element_type=jnp.float32
    )
    return (gate_new[None], up_new[None], down_new[None], mixed.astype(jnp.bfloat16))


def solution(mesh):
    in_specs = (
        P(("grp", "tp"), None),
        P(("grp", "tp"), None),
        P(("grp", "tp"), None),
        P("fs"),
        P("tp", "fs", None),
        P("tp", "fs", None),
        P("tp", None, "fs"),
    )
    out_specs = (
        P(("grp", "tp"), None, "fs"),
        P(("grp", "tp"), None, "fs"),
        P(("grp", "tp"), "fs", None),
        P(("grp", "tp"), "fs"),
    )
    return jax.shard_map(shards, mesh=mesh, in_specs=in_specs, out_specs=out_specs, check_vma=False)
```

```python
import functools
import jax
import jax.numpy as jnp
from jax import lax
from jax.experimental import pallas as pl
from jax.experimental.pallas import tpu as pltpu
from jax.sharding import PartitionSpec as P

EXPERTS = 4
CAP = 128
MESH = pl.DeviceIdType.MESH


def exchange_kernel(F, T, R, C, Q, NEAR, OUT, FINE, gt, ut, dt, gain_at, tokens_at, routes_at, weight_at, gw, uw, dw, mown, mrecv,
                    gain, tokens, routes_t, weight_t, flat, turned, scale_at, wide, tall, sendw, sendt, normed, xs, bh, bl,
                    arr, gacc, uacc, hid, pbf, ret, msend, shared,
                    zs, zr, zt, ys, yr, yt, ts, ps, pr, ms, mr, loc, first):
    g, f, t = lax.axis_index("grp"), lax.axis_index("fs"), lax.axis_index("tp")
    H = R // 2
    wins = (gw, uw, dw)
    low = 1 - lax.div(f, 2)
    inner = lax.rem(lax.div(f + 1, 2), 2)
    near = f + 1 - 2 * lax.rem(f, 2)
    far_in = 1 + low
    far_out = 3 * low
    peers = [lax.rem(t + d, T) for d in range(1, T)]
    others = [near, far_in, far_out]
    far = [far_out, far_in]

    def pick(if_inner, if_outer):
        return inner * if_inner + (1 - inner) * if_outer

    targets = (
        (pick(far_out, near), far_in, pick(near, far_out)),
        (near, far_in, far_out),
        (near, pick(far_out, far_in), pick(far_in, far_out)),
    )
    places = (
        (pick(2, 0), pick(2, 1), pick(0, 1)),
        (0, pick(2, 1), pick(2, 1)),
    )
    items = (
        (0, pick(near, far_in), pick(0, 2)), (0, pick(far_in, near), pick(2, 0)), (1, near, 0),
        (0, far_out, 1), (1, pick(far_in, far_out), pick(2, 1)), (1, pick(far_out, far_in), pick(1, 2)),
    )

    barrier = pltpu.get_barrier_semaphore()
    for p in peers:
        pl.semaphore_signal(barrier, inc=1, device_id={"tp": p}, device_id_type=MESH)
    for p in others:
        pl.semaphore_signal(barrier, inc=1, device_id={"fs": p}, device_id_type=MESH)
    pl.semaphore_signal(barrier, inc=1, device_id={"grp": 1 - g}, device_id_type=MESH)

    def cols_of(src, half):
        return pl.ds(pl.multiple_of(src * R + half * H, H), H)

    def half_cols(half):
        return pl.ds(pl.multiple_of(half * H, H), H)

    W = H // 2
    WIDE = [(n * (H // Q), H // Q, 0, C) for n in range(Q)]
    TALL = [[(n * (C // m), C // m, 0, H) for n in range(m)] for m in (NEAR, OUT)]
    TALL.append([(n * (C // FINE), C // FINE, m * W, W) for m in range(2) for n in range(FINE)])
    BASE = [0, len(TALL[0]), len(TALL[0]) + len(TALL[1])]

    def part(a, src, half, piece):
        row, rows, col, cols = piece
        if a < 2:
            return wins[a].at[pl.ds(pl.multiple_of(src * R + half * H + row, rows), rows), :]
        return dw.at[pl.ds(row, rows), pl.ds(pl.multiple_of(src * R + half * H + col, W), cols)]

    def z_copy(a, k, piece, sem):
        row, rows, col, cols = piece
        held = sendw.at[a, k, pl.ds(row, rows), :] if a < 2 else sendt.at[k, pl.ds(row, rows), pl.ds(col, cols)]
        return pltpu.make_async_remote_copy(
            src_ref=held, dst_ref=part(a, f, g, piece), send_sem=zs.at[min(a, 2) // 2], recv_sem=sem,
            device_id={"fs": targets[a][k]}, device_id_type=MESH)

    def z_send(a, k, place=None):
        if a < 2:
            for q, piece in enumerate(WIDE):
                z_copy(a, k, piece, zr.at[a, places[a][k], q]).start()
        else:
            for q, piece in enumerate(TALL[place]):
                z_copy(a, k, piece, zt.at[BASE[place] + q]).start()

    def z_recv(a, src, piece, sem):
        here = part(a, src, g, piece)
        return pltpu.make_async_remote_copy(
            src_ref=here, dst_ref=here, send_sem=zs.at[min(a, 2) // 2], recv_sem=sem,
            device_id={"fs": src}, device_id_type=MESH)

    def y_copy(a, src, half, piece, sem):
        here = part(a, src, half, piece)
        return pltpu.make_async_remote_copy(
            src_ref=here, dst_ref=here, send_sem=ys.at[a], recv_sem=sem,
            device_id={"grp": 1 - g}, device_id_type=MESH)

    def sent(ref, sem):
        pltpu.make_async_remote_copy(
            src_ref=ref, dst_ref=ref, send_sem=sem, recv_sem=sem,
            device_id={"fs": near}, device_id_type=MESH).wait_send()

    def received(ref, sem):
        pltpu.make_async_remote_copy(
            src_ref=ref, dst_ref=ref, send_sem=sem, recv_sem=sem,
            device_id={"fs": near}, device_id_type=MESH).wait_recv()

    def slots(q):
        return pl.ds(pl.multiple_of(q * CAP, CAP), CAP)

    def t_copy(tgt, src):
        return pltpu.make_async_remote_copy(
            src_ref=xs.at[slots(tgt), :], dst_ref=arr.at[slots(src), :], send_sem=ts.at[0], recv_sem=ts.at[1],
            device_id={"tp": tgt}, device_id_type=MESH)

    def unit(half, chunk):
        if chunk is None:
            return half_cols(half)
        return pl.ds(pl.multiple_of(half * H + chunk * W, W), W)

    def unit_of(c, half, chunk):
        if chunk is None:
            return cols_of(c, half)
        return pl.ds(pl.multiple_of(c * R + half * H + chunk * W, W), W)

    def p_copy(c, kind, half, chunk, tgt, src):
        cols = unit_of(c, half, chunk)
        return pltpu.make_async_remote_copy(
            src_ref=pbf.at[slots(tgt), cols], dst_ref=ret.at[slots(src), cols],
            send_sem=ps.at[0], recv_sem=pr.at[kind + (chunk or 0), half],
            device_id={"tp": tgt}, device_id_type=MESH)

    def near_copy(half):
        return pltpu.make_async_remote_copy(
            src_ref=msend.at[:, cols_of(near, half)], dst_ref=mrecv.at[0, :, half_cols(half)],
            send_sem=ms.at[0], recv_sem=mr.at[0], device_id={"fs": near}, device_id_type=MESH)

    def share_copy(n, half):
        return pltpu.make_async_remote_copy(
            src_ref=msend.at[:, cols_of(far[n], half)], dst_ref=shared.at[n, :, half_cols(half)],
            send_sem=ms.at[1 + n], recv_sem=mr.at[2 + n], device_id={"fs": near}, device_id_type=MESH)

    def cross_copy(n, half, chunk):
        return pltpu.make_async_remote_copy(
            src_ref=msend.at[:, unit_of(far[n], half, chunk)], dst_ref=mrecv.at[1, :, unit(half, chunk)],
            send_sem=ms.at[1 + n], recv_sem=mr.at[1], device_id={"fs": far[n]}, device_id_type=MESH)

    tasks = [(a, k, g) for a in range(3) for k in range(3)]
    tasks += [(a, None, half) for a in range(3) for half in range(2)]

    def stage_copy(n):
        a, k, half = tasks[n]
        tgt = f if k is None else targets[a][k]
        rows, cols = half_cols(half), pl.ds(pl.multiple_of(tgt * C, C), C)
        if a < 2:
            return pltpu.make_async_copy((gt, ut)[a].at[rows, cols], wide.at[n % 3], loc.at[n % 3])
        return pltpu.make_async_copy(dt.at[cols, rows], tall.at[n % 3], loc.at[3 + n % 3])

    def cast_wide(n, begin, end):
        a, k, half = tasks[n]

        @pl.loop(begin // 32, end // 32)
        def _(m):
            rows = pl.ds(pl.multiple_of(m * 32, 32), 32)
            scale = scale_at[pl.ds(pl.multiple_of(half * H + m * 32, 32), 32), 0:1]
            value = (wide[n % 3, rows, :] * scale).astype(jnp.bfloat16)
            if k is None:
                wins[a][pl.ds(pl.multiple_of(f * R + half * H + m * 32, 32), 32), :] = value
            else:
                sendw[a, k, rows, :] = value

    def cast(n):
        a, k, half = tasks[n]
        stage_copy(n).wait()
        if a < 2:
            cast_wide(n, 0, H)
        else:
            @pl.loop(0, C // 128)
            def _(m):
                rows = pl.ds(pl.multiple_of(m * 128, 128), 128)
                value = tall[n % 3, rows, :].astype(jnp.bfloat16)
                if k is None:
                    dw[rows, cols_of(f, half)] = value
                else:
                    sendt[k, rows, :] = value
        if n + 3 < len(tasks):
            stage_copy(n + 3).start()

    def route():
        tok, slot_all = tokens.shape[0], arr.shape[0]

        @pl.loop(0, tok // 32)
        def _(m):
            rows = pl.ds(pl.multiple_of(m * 32, 32), 32)
            value = tokens[rows, :].astype(jnp.float32)
            normed[rows, :] = (
                value * lax.rsqrt(jnp.mean(value * value, axis=-1, keepdims=True) + 1e-06)
            ).astype(jnp.bfloat16)

        one, two = routes_t[0:1, :], routes_t[1:2, :]
        row = lax.broadcasted_iota(jnp.int32, (tok, tok), 0)
        col = lax.broadcasted_iota(jnp.int32, (tok, tok), 1)
        expert = lax.broadcasted_iota(jnp.int32, (16, tok), 0)
        hot = jnp.where((expert == one) | (expert == two), 1.0, 0.0).astype(jnp.bfloat16)
        before = jnp.dot(hot, jnp.where(row < col, 1.0, 0.0).astype(jnp.bfloat16), preferred_element_type=jnp.float32)
        first, second = [
            name.astype(jnp.float32) * CAP
            + jnp.sum(jnp.where(expert == name, before, 0.0), axis=0, keepdims=True)
            for name in (one, two)
        ]
        slot = lax.broadcasted_iota(jnp.int32, (slot_all, tok), 0).astype(jnp.float32)
        select = jnp.where((slot == first) | (slot == second), 1.0, 0.0).astype(jnp.bfloat16)
        for n in range(4):
            cols = pl.ds(n * (F * R // 4), F * R // 4)
            xs[:, cols] = jnp.dot(select, normed[:, cols], preferred_element_type=jnp.float32).astype(jnp.bfloat16)
        flat[...] = jnp.zeros_like(flat)
        for n, line in enumerate((first, second, weight_t[0:1, :], weight_t[1:2, :])):
            flat[n:n + 1, 0:tok] = line
        turned[...] = flat[...].T
        slot = lax.broadcasted_iota(jnp.int32, (tok, slot_all), 1).astype(jnp.float32)
        blend = jnp.where(slot == turned[0:tok, 0:1], turned[0:tok, 2:3], 0.0) + jnp.where(
            slot == turned[0:tok, 1:2], turned[0:tok, 3:4], 0.0)
        high = blend.astype(jnp.bfloat16)
        bh[...] = high
        bl[...] = (blend - high.astype(jnp.float32)).astype(jnp.bfloat16)

    def first_copy(q):
        rows = pl.ds(pl.multiple_of(g * H + q * (H // Q), H // Q), H // Q)
        cols = pl.ds(pl.multiple_of(targets[0][0] * C, C), C)
        return pltpu.make_async_copy(gt.at[rows, cols], wide.at[0, pl.ds(q * (H // Q), H // Q), :], first.at[q])

    small = [pltpu.make_async_copy(a, b, first.at[Q + n]) for n, (a, b) in enumerate(
        ((gain_at, gain), (tokens_at, tokens), (routes_at, routes_t), (weight_at, weight_t)))]
    small[0].start()
    for q in range(Q):
        first_copy(q).start()
    for n in range(1, 3):
        stage_copy(n).start()
    for copy in small[1:]:
        copy.start()
    small[0].wait()
    for n in range(R // 128):
        piece = pl.ds(n * 128, 128)
        scale_at[piece, :] = jnp.broadcast_to(gain[0:1, piece], (128, 128)).T
    for q in range(Q):
        first_copy(q).wait()
        cast_wide(0, q * (H // Q), (q + 1) * (H // Q))
        if q == 0:
            pl.semaphore_wait(barrier, len(peers) + len(others) + 1)
        else:
            z_copy(0, 0, WIDE[q - 1], zr.at[0, places[0][0], q - 1]).start()
    stage_copy(3).start()
    for n in range(1, 9):
        cast(n)
        a, k = tasks[n - 1][:2]
        if n == 1:
            z_copy(0, 0, WIDE[Q - 1], zr.at[0, places[0][0], Q - 1]).start()
        elif n < 8:
            @pl.when(inner == 1)
            def _():
                z_send(a, k, 0)
        else:
            @pl.when(inner == 1)
            def _():
                z_send(2, 1, 2)

            @pl.when(inner == 0)
            def _():
                for pair in ((1, 0), (2, 0), (0, 1), (0, 2), (1, 1), (1, 2)):
                    z_send(*pair, 0)
    for copy in small[1:]:
        copy.wait()
    route()

    @pl.when(inner == 1)
    def _():
        z_send(2, 2, 2)

    for n in range(9, len(tasks)):
        cast(n)
        if n == 9:
            for p in peers:
                t_copy(p, t).start()
    arr[slots(t), :] = xs[slots(t), :]

    rows_all = arr.shape[0]
    M = min(256, rows_all)

    def multiply(a, src, first):
        acc = (gacc, uacc)[a]
        deep = pl.ds(pl.multiple_of(src * R, R), R)

        @pl.loop(0, rows_all // M)
        def _(m):
            rows = pl.ds(pl.multiple_of(m * M, M), M)
            value = jnp.dot(arr[rows, deep], wins[a][deep, :], preferred_element_type=jnp.float32)
            if first:
                acc[rows, :] = value
            else:
                acc[rows, :] += value

    def activate():
        @pl.loop(0, rows_all // 64)
        def _(m):
            rows = pl.ds(pl.multiple_of(m * 64, 64), 64)
            v = gacc[rows, :]
            hid[rows, :] = (v / (1.0 + jnp.exp(-v)) * uacc[rows, :]).astype(jnp.bfloat16)

    def partial_out(c, kind, half, chunk=None):
        cols = unit_of(c, half, chunk)

        @pl.loop(0, rows_all // M)
        def _(m):
            rows = pl.ds(pl.multiple_of(m * M, M), M)
            pbf[rows, cols] = jnp.dot(hid[rows, :], dw[:, cols], preferred_element_type=jnp.float32).astype(jnp.bfloat16)

        for p in peers:
            p_copy(c, kind, half, chunk, p, t).start()
        ret[slots(t), cols] = pbf[slots(t), cols]

    def mix(c, kind, half, chunk=None):
        cols = unit_of(c, half, chunk)
        received(ret.at[pl.ds(0, len(peers) * CAP), cols], pr.at[kind + (chunk or 0), half])
        return jnp.dot(bh[...], ret[:, cols], preferred_element_type=jnp.float32) + jnp.dot(
            bl[...], ret[:, cols], preferred_element_type=jnp.float32)

    def mix_own(half):
        mown[:, half_cols(half)] = mix(f, 0, half)

    def mix_near(half):
        msend[:, cols_of(near, half)] = mix(near, 1, half).astype(jnp.bfloat16)
        near_copy(half).start()

    def join(n, half, chunk=None):
        cols = unit_of(far[n], half, chunk)
        both = mix(far[n], 2 + n, half, chunk) + shared[n, :, unit(half, chunk)].astype(jnp.float32)
        msend[:, cols] = both.astype(jnp.bfloat16)
        cross_copy(n, half, chunk).start()

    def share(n, half):
        msend[:, cols_of(far[n], half)] = mix(far[n], 2 + n, half).astype(jnp.bfloat16)
        share_copy(n, half).start()

    def stream(a, place):
        if a < 2:
            return [(piece, zr.at[a, place, q], yr.at[a, place, q]) for q, piece in enumerate(WIDE)]
        return [(piece, zt.at[BASE[place] + q], yt.at[BASE[place] + q]) for q, piece in enumerate(TALL[place])]

    def forward(a, src, place, begin, end):
        for piece, z, y in stream(a, place)[begin:end]:
            z_recv(a, src, piece, z).wait_recv()
            y_copy(a, src, g, piece, y).start()

    def landed(a, src, place, begin=0, end=None):
        for piece, _, y in stream(a, place)[begin:end]:
            y_copy(a, src, 1 - g, piece, y).wait_recv()

    def settle(a, src, place):
        landed(a, src, place)
        multiply(a, src, False)

    half_way = Q // 2
    forward(*items[0], 0, Q)
    forward(*items[1], 0, Q)
    received(xs.at[pl.ds(0, len(peers) * CAP), :], ts.at[1])
    for a in (0, 1):
        multiply(a, f, True)
    for n in range(2, 6):
        forward(*items[n], 0, half_way)
        settle(*items[n - 2])
        forward(*items[n], half_way, Q)
    settle(*items[4])

    @pl.when(inner == 0)
    def _():
        z_send(2, 1, 1)
        z_send(2, 2, 1)

    forward(2, near, 0, 0, NEAR)
    settle(*items[5])
    activate()
    partial_out(f, 0, 0)
    partial_out(f, 0, 1)
    partial_out(near, 1, g)
    landed(2, near, 0)
    partial_out(near, 1, 1 - g)
    mix_own(0)
    mix_own(1)
    mix_near(g)
    forward(2, far_out, 1, 0, 1)
    mix_near(1 - g)
    forward(2, far_out, 1, 1, OUT)
    partial_out(far_out, 2, g)

    def forward_in(begin, end):
        forward(2, far_in, 2, begin, end)

    @pl.when(inner == 0)
    def _():
        forward_in(0, FINE)
        landed(2, far_out, 1)
        partial_out(far_out, 2, 1 - g)
        forward_in(FINE, 2 * FINE)
        share(0, g)
        share(0, 1 - g)
        partial_out(far_in, 3, g)
        landed(2, far_in, 2)
        partial_out(far_in, 3, 1 - g)
        share(1, g)
        share(1, 1 - g)

    @pl.when(inner == 1)
    def _():
        landed(2, far_out, 1)
        partial_out(far_out, 2, 1 - g)
        forward_in(0, FINE)
        partial_out(far_in, 3, g, 0)
        forward_in(FINE, FINE + 1)
        landed(2, far_in, 2, 0, FINE)
        partial_out(far_in, 3, 1 - g, 0)
        forward_in(FINE + 1, 2 * FINE)
        partial_out(far_in, 3, g, 1)
        received(shared.at[0], mr.at[2])
        join(0, g)
        join(0, 1 - g)
        received(shared.at[1], mr.at[3])
        join(1, g, 0)
        join(1, 1 - g, 0)
        landed(2, far_in, 2, FINE, 2 * FINE)
        partial_out(far_in, 3, 1 - g, 1)
        join(1, g, 1)
        join(1, 1 - g, 1)

    sent(xs.at[pl.ds(0, len(peers) * CAP), :], ts.at[0])
    sent(sendw, zs.at[0])
    sent(sendt, zs.at[1])
    for a in range(3):
        sent(sendw.at[a] if a < 2 else sendt, ys.at[a])
    sent(pbf.at[pl.ds(0, len(peers) * CAP), :], ps.at[0])
    received(mrecv.at[0], mr.at[0])
    received(mrecv.at[1], mr.at[1])
    for n in range(3):
        sent(msend.at[:, pl.ds(0, R)], ms.at[n])


def deliver_kernel(gw, uw, dw, mown, mrecv, go, uo, do, mo, total, sems):
    copies = [pltpu.make_async_copy(a, b, sems.at[n]) for n, (a, b) in enumerate(((gw, go), (uw, uo), (dw, do)))]
    for copy in copies:
        copy.start()
    value = mown[...]
    for n in range(mrecv.shape[0]):
        value = value + mrecv[n].astype(jnp.float32)
    total[...] = value.astype(jnp.bfloat16)
    last = pltpu.make_async_copy(total, mo, sems.at[len(copies)])
    last.start()
    for copy in copies + [last]:
        copy.wait()


def exchange(F, T, gate, up, down, gain, tokens, routes, weight):
    span = -(-tokens.shape[0] // 128) * 128
    R, FF = gate.shape
    C, D, H = FF // F, F * R, R // 2
    Q, NEAR, OUT, FINE = 4, 2, 4, 4
    tok, S = tokens.shape[0], EXPERTS * CAP
    bf, f32 = jnp.bfloat16, jnp.float32
    any_spec, vm = pl.BlockSpec(memory_space=pl.ANY), pl.BlockSpec(memory_space=pltpu.VMEM)
    dma = pltpu.SemaphoreType.DMA
    held = pl.pallas_call(
        functools.partial(exchange_kernel, F, T, R, C, Q, NEAR, OUT, FINE),
        name="exchange",
        out_shape=(pltpu.VMEM((D, C), bf), pltpu.VMEM((D, C), bf), pltpu.VMEM((C, D), bf),
                   pltpu.VMEM((tok, R), f32), pltpu.VMEM((2, tok, R), bf)),
        in_specs=[any_spec] * 7,
        out_specs=(vm,) * 5,
        scratch_shapes=[
            pltpu.VMEM((1, R), f32), pltpu.VMEM((tok, D), bf), pltpu.VMEM((routes.shape[1], tok), jnp.int32),
            pltpu.VMEM((routes.shape[1], tok), f32), pltpu.VMEM((128, span), f32), pltpu.VMEM((span, 128), f32), pltpu.VMEM((R, 128), f32),
            pltpu.VMEM((3, H, C), f32), pltpu.VMEM((3, C, H), f32),
            pltpu.VMEM((2, F - 1, H, C), bf), pltpu.VMEM((F - 1, C, H), bf),
            pltpu.VMEM((tok, D), bf), pltpu.VMEM((S, D), bf), pltpu.VMEM((tok, S), bf), pltpu.VMEM((tok, S), bf),
            pltpu.VMEM((S, D), bf),
            pltpu.VMEM((S, C), f32), pltpu.VMEM((S, C), f32), pltpu.VMEM((S, C), bf),
            pltpu.VMEM((S, D), bf), pltpu.VMEM((S, D), bf), pltpu.VMEM((tok, D), bf), pltpu.VMEM((2, tok, R), bf),
            dma((2,)), dma((2, F - 1, Q)), dma((NEAR + OUT + 2 * FINE,)), dma((3,)), dma((2, F - 1, Q)), dma((NEAR + OUT + 2 * FINE,)), dma((2,)),
            dma((1,)), dma((5, 2)), dma((3,)), dma((4,)), dma((6,)), dma((Q + 4,)),
        ],
        compiler_params=pltpu.CompilerParams(collective_id=0, has_side_effects=True, vmem_limit_bytes=42 * 1024 * 1024),
    )(gate, up, down, gain[None, :], tokens, routes.T, weight.T)
    return pl.pallas_call(
        deliver_kernel,
        name="deliver",
        out_shape=(jax.ShapeDtypeStruct((D, C), bf), jax.ShapeDtypeStruct((D, C), bf),
                   jax.ShapeDtypeStruct((C, D), bf), jax.ShapeDtypeStruct((tok, R), bf)),
        in_specs=[vm] * 5,
        out_specs=(pl.BlockSpec(memory_space=pltpu.HBM),) * 4,
        scratch_shapes=[pltpu.VMEM((tok, R), bf), dma((4,))],
        compiler_params=pltpu.CompilerParams(vmem_limit_bytes=4 * 1024 * 1024),
    )(*[pltpu.with_memory_space_constraint(x, pltpu.VMEM) for x in held])


def fits(grp_count, fs_count, pieces, gate_train):
    rows, wide = gate_train.shape[1:]
    return (grp_count == 2 and fs_count == pieces and fs_count == 4
            and wide % (fs_count * 128) == 0 and rows % 256 == 0)


def shards(tokens, routes, route_weight, norm_gain, gate_train, up_train, down_train):
    fs_count = lax.axis_size("fs")
    pieces = min(fs_count, 32)
    copies = fs_count // pieces
    if fits(lax.axis_size("grp"), fs_count, pieces, gate_train):
        gate_new, up_new, down_new, mixed = exchange(
            fs_count, lax.axis_size("tp"), gate_train[0], up_train[0], down_train[0],
            norm_gain, tokens, routes, route_weight,
        )
        return (gate_new[None], up_new[None], down_new[None], mixed)
    gain_column = norm_gain[:, None]
    gate_low = (gate_train[0] * gain_column).astype(jnp.bfloat16)
    up_low = (up_train[0] * gain_column).astype(jnp.bfloat16)
    down_low = down_train[0].astype(jnp.bfloat16)
    gate_wide = jnp.tile(gate_low, (1, copies))
    up_wide = jnp.tile(up_low, (1, copies))
    down_wide = jnp.tile(down_low, (copies, 1))
    gate_new, up_new = (
        lax.all_to_all(gate_wide, "fs", split_axis=1, concat_axis=0, tiled=True),
        lax.all_to_all(up_wide, "fs", split_axis=1, concat_axis=0, tiled=True),
    )
    down_new = lax.all_to_all(down_wide, "fs", split_axis=0, concat_axis=1, tiled=True)
    tok_float = tokens.astype(jnp.float32)
    normed = (
        tok_float * lax.rsqrt(jnp.mean(tok_float * tok_float, axis=-1, keepdims=True) + 1e-06)
    ).astype(jnp.bfloat16)
    chosen = routes.reshape(-1)
    chosen_hot = (chosen[:, None] == jnp.arange(EXPERTS, dtype=jnp.int32)[None, :]).astype(
        jnp.int32
    )
    before = jnp.cumsum(chosen_hot, axis=0) - chosen_hot
    slot_rank = jnp.sum(before * chosen_hot, axis=1)
    slot_index = (chosen * CAP + slot_rank).reshape(routes.shape)
    slot_range = jnp.arange(EXPERTS * CAP, dtype=jnp.int32)
    select_rows = jnp.any(slot_range[:, None, None] == slot_index[None, :, :], axis=-1).astype(
        jnp.bfloat16
    )
    outgoing = jnp.dot(select_rows, normed, preferred_element_type=jnp.float32).astype(jnp.bfloat16)
    outgoing = outgoing.reshape(EXPERTS, CAP, normed.shape[1])
    arrived = lax.all_to_all(outgoing, "tp", split_axis=0, concat_axis=0, tiled=True).reshape(
        EXPERTS * CAP, normed.shape[1]
    )
    slot_count = EXPERTS * CAP // copies
    copy_index = lax.axis_index("fs") // pieces
    my_rows = lax.dynamic_slice_in_dim(arrived, copy_index * slot_count, slot_count, 0)
    gated = jnp.dot(my_rows, gate_new, preferred_element_type=jnp.float32)
    lifted = jnp.dot(my_rows, up_new, preferred_element_type=jnp.float32)
    hidden = (jax.nn.silu(gated) * lifted).astype(jnp.bfloat16)
    partial_out = jnp.dot(hidden, down_new, preferred_element_type=jnp.float32)
    placed = jnp.zeros((EXPERTS * CAP, partial_out.shape[1]), jnp.float32)
    placed = lax.dynamic_update_slice_in_dim(placed, partial_out, copy_index * slot_count, 0)
    expert_out = lax.psum_scatter(placed, "fs", scatter_dimension=1, tiled=True).astype(
        jnp.bfloat16
    )
    returned = lax.all_to_all(
        expert_out.reshape(EXPERTS, CAP, expert_out.shape[1]),
        "tp",
        split_axis=0,
        concat_axis=0,
        tiled=True,
    )
    returned = returned.reshape(EXPERTS * CAP, expert_out.shape[1]).astype(jnp.float32)
    blend_weight = jnp.sum(
        jnp.where(
            slot_range[None, None, :] == slot_index[:, :, None], route_weight[:, :, None], 0.0
        ),
        axis=1,
    )
    mixed = jnp.dot(
        blend_weight, returned, precision=lax.Precision.HIGHEST, preferred_element_type=jnp.float32
    )
    return (gate_new[None], up_new[None], down_new[None], mixed.astype(jnp.bfloat16))


def solution(mesh):
    in_specs = (
        P(("grp", "tp"), None),
        P(("grp", "tp"), None),
        P(("grp", "tp"), None),
        P("fs"),
        P("tp", "fs", None),
        P("tp", "fs", None),
        P("tp", None, "fs"),
    )
    out_specs = (
        P(("grp", "tp"), None, "fs"),
        P(("grp", "tp"), None, "fs"),
        P(("grp", "tp"), "fs", None),
        P(("grp", "tp"), "fs"),
    )
    return jax.shard_map(shards, mesh=mesh, in_specs=in_specs, out_specs=out_specs, check_vma=False)
```

```python
import functools
import jax
import jax.numpy as jnp
from jax import lax
from jax.experimental import pallas as pl
from jax.experimental.pallas import tpu as pltpu
from jax.sharding import PartitionSpec as P

EXPERTS = 4
CAP = 128
MESH = pl.DeviceIdType.MESH


def exchange_kernel(F, T, R, C, Q, NEAR, OUT, FINE, gt, ut, dt, gain_at, tokens_at, routes_at, weight_at, gw, uw, dw, mown, mrecv,
                    gain, tokens, routes_t, weight_t, flat, turned, scale_at, wide, tall, sendw, sendt, normed, xs, bh, bl,
                    early, arr, gacc, uacc, hid, pbf, ret, msend, shared,
                    zs, zr, zt, ys, yr, yt, ts, ps, pr, ms, mr, loc):
    g, f, t = lax.axis_index("grp"), lax.axis_index("fs"), lax.axis_index("tp")
    H = R // 2
    wins = (gw, uw, dw)
    low = 1 - lax.div(f, 2)
    inner = lax.rem(lax.div(f + 1, 2), 2)
    near = f + 1 - 2 * lax.rem(f, 2)
    far_in = 1 + low
    far_out = 3 * low
    peers = [lax.rem(t + d, T) for d in range(1, T)]
    others = [near, far_in, far_out]
    far = [far_out, far_in]

    def pick(if_inner, if_outer):
        return inner * if_inner + (1 - inner) * if_outer

    targets = (
        (pick(far_out, near), far_in, pick(near, far_out)),
        (near, far_in, far_out),
        (near, pick(far_out, far_in), pick(far_in, far_out)),
    )
    places = (
        (pick(2, 0), pick(2, 1), pick(0, 1)),
        (0, pick(2, 1), pick(2, 1)),
    )
    items = (
        (0, pick(near, far_in), pick(0, 2)), (0, pick(far_in, near), pick(2, 0)), (1, near, 0),
        (0, far_out, 1), (1, pick(far_in, far_out), pick(2, 1)), (1, pick(far_out, far_in), pick(1, 2)),
    )

    barrier = pltpu.get_barrier_semaphore()
    for p in peers:
        pl.semaphore_signal(barrier, inc=1, device_id={"tp": p}, device_id_type=MESH)
    for p in others:
        pl.semaphore_signal(barrier, inc=1, device_id={"fs": p}, device_id_type=MESH)
    pl.semaphore_signal(barrier, inc=1, device_id={"grp": 1 - g}, device_id_type=MESH)

    def cols_of(src, half):
        return pl.ds(pl.multiple_of(src * R + half * H, H), H)

    def half_cols(half):
        return pl.ds(pl.multiple_of(half * H, H), H)

    W = H // 2
    WIDE = [(n * (H // Q), H // Q, 0, C) for n in range(Q)]
    TALL = [[(n * (C // m), C // m, 0, H) for n in range(m)] for m in (NEAR, OUT)]
    TALL.append([(n * (C // FINE), C // FINE, m * W, W) for m in range(2) for n in range(FINE)])
    ALL = len(TALL[2])
    BASE = [0, len(TALL[0]), len(TALL[0]) + len(TALL[1])]

    def part(a, src, half, piece):
        row, rows, col, cols = piece
        if a < 2:
            return wins[a].at[pl.ds(pl.multiple_of(src * R + half * H + row, rows), rows), :]
        return dw.at[pl.ds(row, rows), pl.ds(pl.multiple_of(src * R + half * H + col, W), cols)]

    def z_copy(a, k, piece, sem):
        row, rows, col, cols = piece
        held = sendw.at[a, k, pl.ds(row, rows), :] if a < 2 else sendt.at[k, pl.ds(row, rows), pl.ds(col, cols)]
        return pltpu.make_async_remote_copy(
            src_ref=held, dst_ref=part(a, f, g, piece), send_sem=zs.at[min(a, 2) // 2], recv_sem=sem,
            device_id={"fs": targets[a][k]}, device_id_type=MESH)

    def z_send(a, k, place=None):
        if a < 2:
            for q, piece in enumerate(WIDE):
                z_copy(a, k, piece, zr.at[a, places[a][k], q]).start()
        else:
            for q, piece in enumerate(TALL[place]):
                z_copy(a, k, piece, zt.at[BASE[place] + q]).start()

    def z_recv(a, src, piece, sem):
        here = part(a, src, g, piece)
        return pltpu.make_async_remote_copy(
            src_ref=here, dst_ref=here, send_sem=zs.at[min(a, 2) // 2], recv_sem=sem,
            device_id={"fs": src}, device_id_type=MESH)

    def y_copy(a, src, half, piece, sem):
        here = part(a, src, half, piece)
        return pltpu.make_async_remote_copy(
            src_ref=here, dst_ref=here, send_sem=ys.at[a], recv_sem=sem,
            device_id={"grp": 1 - g}, device_id_type=MESH)

    def sent(ref, sem):
        pltpu.make_async_remote_copy(
            src_ref=ref, dst_ref=ref, send_sem=sem, recv_sem=sem,
            device_id={"fs": near}, device_id_type=MESH).wait_send()

    def received(ref, sem):
        pltpu.make_async_remote_copy(
            src_ref=ref, dst_ref=ref, send_sem=sem, recv_sem=sem,
            device_id={"fs": near}, device_id_type=MESH).wait_recv()

    def slots(q):
        return pl.ds(pl.multiple_of(q * CAP, CAP), CAP)

    def t_copy(tgt, src):
        return pltpu.make_async_remote_copy(
            src_ref=xs.at[slots(tgt), :], dst_ref=arr.at[slots(src), :], send_sem=ts.at[0], recv_sem=ts.at[1],
            device_id={"tp": tgt}, device_id_type=MESH)

    def unit(half, chunk):
        if chunk is None:
            return half_cols(half)
        return pl.ds(pl.multiple_of(half * H + chunk * W, W), W)

    def unit_of(c, half, chunk):
        if chunk is None:
            return cols_of(c, half)
        return pl.ds(pl.multiple_of(c * R + half * H + chunk * W, W), W)

    def p_copy(c, kind, half, chunk, tgt, src):
        cols = unit_of(c, half, chunk)
        return pltpu.make_async_remote_copy(
            src_ref=pbf.at[slots(tgt), cols], dst_ref=ret.at[slots(src), cols],
            send_sem=ps.at[0], recv_sem=pr.at[kind + (chunk or 0), half],
            device_id={"tp": tgt}, device_id_type=MESH)

    def near_copy(half):
        return pltpu.make_async_remote_copy(
            src_ref=msend.at[:, cols_of(near, half)], dst_ref=mrecv.at[0, :, half_cols(half)],
            send_sem=ms.at[0], recv_sem=mr.at[0], device_id={"fs": near}, device_id_type=MESH)

    def share_copy(n, half):
        return pltpu.make_async_remote_copy(
            src_ref=msend.at[:, cols_of(far[n], half)], dst_ref=shared.at[n, :, half_cols(half)],
            send_sem=ms.at[1 + n], recv_sem=mr.at[2 + n], device_id={"fs": near}, device_id_type=MESH)

    def cross_copy(n, half, chunk):
        return pltpu.make_async_remote_copy(
            src_ref=msend.at[:, unit_of(far[n], half, chunk)], dst_ref=mrecv.at[1, :, unit(half, chunk)],
            send_sem=ms.at[1 + n], recv_sem=mr.at[1], device_id={"fs": far[n]}, device_id_type=MESH)

    tasks = [(a, k, g) for a in range(3) for k in range(3)]
    tasks += [(a, None, half) for a in range(3) for half in range(2)]

    def stage_copy(n):
        a, k, half = tasks[n]
        tgt = f if k is None else targets[a][k]
        rows, cols = half_cols(half), pl.ds(pl.multiple_of(tgt * C, C), C)
        if a < 2:
            return pltpu.make_async_copy((gt, ut)[a].at[rows, cols], wide.at[n % 3], loc.at[n % 3])
        return pltpu.make_async_copy(dt.at[cols, rows], tall.at[n % 3], loc.at[3 + n % 3])

    def cast_wide(n, begin, end):
        a, k, half = tasks[n]

        @pl.loop(begin // 32, end // 32)
        def _(m):
            rows = pl.ds(pl.multiple_of(m * 32, 32), 32)
            scale = scale_at[pl.ds(pl.multiple_of(half * H + m * 32, 32), 32), 0:1]
            value = (wide[n % 3, rows, :] * scale).astype(jnp.bfloat16)
            if k is None:
                wins[a][pl.ds(pl.multiple_of(f * R + half * H + m * 32, 32), 32), :] = value
            else:
                sendw[a, k, rows, :] = value

    def cast(n):
        a, k, half = tasks[n]
        stage_copy(n).wait()
        if a < 2:
            cast_wide(n, 0, H)
        else:
            @pl.loop(0, C // 128)
            def _(m):
                rows = pl.ds(pl.multiple_of(m * 128, 128), 128)
                value = tall[n % 3, rows, :].astype(jnp.bfloat16)
                if k is None:
                    dw[rows, cols_of(f, half)] = value
                else:
                    sendt[k, rows, :] = value
        if n + 3 < len(tasks):
            stage_copy(n + 3).start()

    def route():
        tok, slot_all = tokens.shape[0], arr.shape[0]

        @pl.loop(0, tok // 32)
        def _(m):
            rows = pl.ds(pl.multiple_of(m * 32, 32), 32)
            value = tokens[rows, :].astype(jnp.float32)
            normed[rows, :] = (
                value * lax.rsqrt(jnp.mean(value * value, axis=-1, keepdims=True) + 1e-06)
            ).astype(jnp.bfloat16)

        one, two = routes_t[0:1, :], routes_t[1:2, :]
        row = lax.broadcasted_iota(jnp.int32, (tok, tok), 0)
        col = lax.broadcasted_iota(jnp.int32, (tok, tok), 1)
        expert = lax.broadcasted_iota(jnp.int32, (16, tok), 0)
        hot = jnp.where((expert == one) | (expert == two), 1.0, 0.0).astype(jnp.bfloat16)
        before = jnp.dot(hot, jnp.where(row < col, 1.0, 0.0).astype(jnp.bfloat16), preferred_element_type=jnp.float32)
        first, second = [
            name.astype(jnp.float32) * CAP
            + jnp.sum(jnp.where(expert == name, before, 0.0), axis=0, keepdims=True)
            for name in (one, two)
        ]
        slot = lax.broadcasted_iota(jnp.int32, (slot_all, tok), 0).astype(jnp.float32)
        select = jnp.where((slot == first) | (slot == second), 1.0, 0.0).astype(jnp.bfloat16)
        for n in range(4):
            cols = pl.ds(n * (F * R // 4), F * R // 4)
            xs[:, cols] = jnp.dot(select, normed[:, cols], preferred_element_type=jnp.float32).astype(jnp.bfloat16)
        flat[...] = jnp.zeros_like(flat)
        for n, line in enumerate((first, second, weight_t[0:1, :], weight_t[1:2, :])):
            flat[n:n + 1, 0:tok] = line
        turned[...] = flat[...].T
        slot = lax.broadcasted_iota(jnp.int32, (tok, slot_all), 1).astype(jnp.float32)
        blend = jnp.where(slot == turned[0:tok, 0:1], turned[0:tok, 2:3], 0.0) + jnp.where(
            slot == turned[0:tok, 1:2], turned[0:tok, 3:4], 0.0)
        high = blend.astype(jnp.bfloat16)
        bh[...] = high
        bl[...] = (blend - high.astype(jnp.float32)).astype(jnp.bfloat16)

    idle = (ps.at[0], ms.at[0], ms.at[1], ms.at[2])

    def first_copy(q):
        rows = pl.ds(pl.multiple_of(g * H + q * (H // Q), H // Q), H // Q)
        cols = pl.ds(pl.multiple_of(targets[0][0] * C, C), C)
        return pltpu.make_async_copy(gt.at[rows, cols], wide.at[0, pl.ds(q * (H // Q), H // Q), :], idle[q])

    small = [pltpu.make_async_copy(a, b, c) for a, b, c in (
        (gain_at, gain, ts.at[0]), (tokens_at, tokens, loc.at[3]),
        (routes_at, routes_t, loc.at[4]), (weight_at, weight_t, loc.at[5]))]
    small[0].start()
    for q in range(Q):
        first_copy(q).start()
    for n in range(1, 3):
        stage_copy(n).start()
    for copy in small[1:]:
        copy.start()
    small[0].wait()
    for n in range(R // 128):
        piece = pl.ds(n * 128, 128)
        scale_at[piece, :] = jnp.broadcast_to(gain[0:1, piece], (128, 128)).T
    for q in range(Q):
        first_copy(q).wait()
        cast_wide(0, q * (H // Q), (q + 1) * (H // Q))
        if q == 0:
            pl.semaphore_wait(barrier, len(peers) + len(others) + 1)
        else:
            z_copy(0, 0, WIDE[q - 1], zr.at[0, places[0][0], q - 1]).start()
    stage_copy(3).start()
    for n in range(1, 9):
        if n == 3:
            for copy in small[1:]:
                copy.wait()
        cast(n)
        a, k = tasks[n - 1][:2]
        if n == 1:
            z_copy(0, 0, WIDE[Q - 1], zr.at[0, places[0][0], Q - 1]).start()
        elif n < 8:
            @pl.when(inner == 1)
            def _():
                z_send(a, k, 0)
        else:
            @pl.when(inner == 1)
            def _():
                z_send(2, 1, 2)

            @pl.when(inner == 0)
            def _():
                for pair in ((1, 0), (2, 0), (0, 1), (0, 2), (1, 1), (1, 2)):
                    z_send(*pair, 0)
    route()

    @pl.when(inner == 1)
    def _():
        z_send(2, 2, 2)

    for n in range(9, len(tasks)):
        cast(n)
        if n == 9:
            for p in peers:
                t_copy(p, t).start()
    arr[slots(t), :] = xs[slots(t), :]

    rows_all = arr.shape[0]
    M = min(256, rows_all)

    def multiply(a, src, first):
        acc = (gacc, uacc)[a]
        deep = pl.ds(pl.multiple_of(src * R, R), R)

        @pl.loop(0, rows_all // M)
        def _(m):
            rows = pl.ds(pl.multiple_of(m * M, M), M)
            value = jnp.dot(arr[rows, deep], wins[a][deep, :], preferred_element_type=jnp.float32)
            if first:
                acc[rows, :] = value
            else:
                acc[rows, :] += value

    def activate():
        @pl.loop(0, rows_all // 64)
        def _(m):
            rows = pl.ds(pl.multiple_of(m * 64, 64), 64)
            v = gacc[rows, :]
            hid[rows, :] = (v / (1.0 + jnp.exp(-v)) * uacc[rows, :]).astype(jnp.bfloat16)

    def partial_out(c, kind, half, chunk=None):
        cols = unit_of(c, half, chunk)

        @pl.loop(0, rows_all // M)
        def _(m):
            rows = pl.ds(pl.multiple_of(m * M, M), M)
            pbf[rows, cols] = jnp.dot(hid[rows, :], dw[:, cols], preferred_element_type=jnp.float32).astype(jnp.bfloat16)

        for p in peers:
            p_copy(c, kind, half, chunk, p, t).start()
        ret[slots(t), cols] = pbf[slots(t), cols]

    def spread(c, kind, half, chunk):
        cols = unit_of(c, half, chunk)
        for p in peers:
            p_copy(c, kind, half, chunk, p, t).start()
        ret[slots(t), cols] = pbf[slots(t), cols]

    def partial_early(half, cut):
        early[...] = jnp.dot(hid[:, 0:cut], dw[0:cut, unit_of(far_in, half, 1)], preferred_element_type=jnp.float32)

    def partial_late(half, cut):
        cols = unit_of(far_in, half, 1)
        value = early[...] + jnp.dot(hid[:, cut:C], dw[cut:C, cols], preferred_element_type=jnp.float32)
        pbf[:, cols] = value.astype(jnp.bfloat16)
        spread(far_in, 3, half, 1)

    def mix(c, kind, half, chunk=None):
        cols = unit_of(c, half, chunk)
        received(ret.at[pl.ds(0, len(peers) * CAP), cols], pr.at[kind + (chunk or 0), half])
        return jnp.dot(bh[...], ret[:, cols], preferred_element_type=jnp.float32) + jnp.dot(
            bl[...], ret[:, cols], preferred_element_type=jnp.float32)

    def mix_own(half):
        mown[:, half_cols(half)] = mix(f, 0, half)

    def mix_near(half):
        msend[:, cols_of(near, half)] = mix(near, 1, half).astype(jnp.bfloat16)
        near_copy(half).start()

    def join(n, half, chunk=None):
        cols = unit_of(far[n], half, chunk)
        both = mix(far[n], 2 + n, half, chunk) + shared[n, :, unit(half, chunk)].astype(jnp.float32)
        msend[:, cols] = both.astype(jnp.bfloat16)
        cross_copy(n, half, chunk).start()

    def share(n, half):
        msend[:, cols_of(far[n], half)] = mix(far[n], 2 + n, half).astype(jnp.bfloat16)
        share_copy(n, half).start()

    def stream(a, place):
        if a < 2:
            return [(piece, zr.at[a, place, q], yr.at[a, place, q]) for q, piece in enumerate(WIDE)]
        return [(piece, zt.at[BASE[place] + q], yt.at[BASE[place] + q]) for q, piece in enumerate(TALL[place])]

    def forward(a, src, place, begin, end):
        for piece, z, y in stream(a, place)[begin:end]:
            z_recv(a, src, piece, z).wait_recv()
            y_copy(a, src, g, piece, y).start()

    def landed(a, src, place, begin=0, end=None):
        for piece, _, y in stream(a, place)[begin:end]:
            y_copy(a, src, 1 - g, piece, y).wait_recv()

    def settle(a, src, place):
        landed(a, src, place)
        multiply(a, src, False)

    half_way = Q // 2
    forward(*items[0], 0, Q)
    forward(*items[1], 0, Q)
    received(xs.at[pl.ds(0, len(peers) * CAP), :], ts.at[1])
    for a in (0, 1):
        multiply(a, f, True)
    for n in range(2, 6):
        forward(*items[n], 0, half_way)
        settle(*items[n - 2])
        forward(*items[n], half_way, Q)
        if n == 3:
            forward(2, near, 0, 0, NEAR)
    settle(*items[4])

    @pl.when(inner == 0)
    def _():
        z_send(2, 2, 1)
        z_send(2, 1, 1)

    settle(*items[5])
    activate()
    partial_out(f, 0, 0)
    partial_out(f, 0, 1)
    partial_out(near, 1, g)
    landed(2, near, 0)
    partial_out(near, 1, 1 - g)
    mix_own(0)
    mix_own(1)
    mix_near(g)
    forward(2, far_out, 1, 0, 1)
    mix_near(1 - g)
    forward(2, far_out, 1, 1, OUT)
    partial_out(far_out, 2, g)

    def forward_in(begin, end):
        forward(2, far_in, 2, begin, end)

    @pl.when(inner == 0)
    def _():
        forward_in(0, FINE)
        landed(2, far_out, 1)
        partial_out(far_out, 2, 1 - g)
        forward_in(FINE, ALL)
        share(0, g)
        share(0, 1 - g)
        partial_out(far_in, 3, g)
        landed(2, far_in, 2)
        partial_out(far_in, 3, 1 - g)
        share(1, g)
        share(1, 1 - g)

    @pl.when(inner == 1)
    def _():
        landed(2, far_out, 1)
        partial_out(far_out, 2, 1 - g)
        forward_in(0, FINE)
        partial_out(far_in, 3, g, 0)
        forward_in(FINE, FINE + FINE // 2)
        landed(2, far_in, 2, 0, FINE)
        partial_out(far_in, 3, 1 - g, 0)
        forward_in(FINE + FINE // 2, ALL - 1)
        received(shared.at[0], mr.at[2])
        join(0, g)
        join(0, 1 - g)
        forward_in(ALL - 1, ALL)
        partial_out(far_in, 3, g, 1)
        received(shared.at[1], mr.at[3])
        join(1, g, 0)
        join(1, 1 - g, 0)
        cut = (ALL - FINE - 1) * C // FINE // 128 * 128
        landed(2, far_in, 2, FINE, ALL - 1)
        partial_early(1 - g, cut)
        landed(2, far_in, 2, ALL - 1, ALL)
        partial_late(1 - g, cut)
        join(1, g, 1)
        join(1, 1 - g, 1)

    sent(xs.at[pl.ds(0, len(peers) * CAP), :], ts.at[0])
    sent(sendw, zs.at[0])
    sent(sendt, zs.at[1])
    for a in range(3):
        sent(sendw.at[a] if a < 2 else sendt, ys.at[a])
    sent(pbf.at[pl.ds(0, len(peers) * CAP), :], ps.at[0])
    received(mrecv.at[0], mr.at[0])
    received(mrecv.at[1], mr.at[1])
    for n in range(3):
        sent(msend.at[:, pl.ds(0, R)], ms.at[n])


def deliver_kernel(gw, uw, dw, mown, mrecv, go, uo, do, mo, total, sems):
    copies = [pltpu.make_async_copy(a, b, sems.at[n]) for n, (a, b) in enumerate(((gw, go), (uw, uo), (dw, do)))]
    for copy in copies:
        copy.start()
    value = mown[...]
    for n in range(mrecv.shape[0]):
        value = value + mrecv[n].astype(jnp.float32)
    total[...] = value.astype(jnp.bfloat16)
    last = pltpu.make_async_copy(total, mo, sems.at[len(copies)])
    last.start()
    for copy in copies + [last]:
        copy.wait()


def exchange(F, T, gate, up, down, gain, tokens, routes, weight):
    span = -(-tokens.shape[0] // 128) * 128
    R, FF = gate.shape
    C, D, H = FF // F, F * R, R // 2
    Q, NEAR, OUT, FINE = 4, 1, 2, 8
    tok, S = tokens.shape[0], EXPERTS * CAP
    bf, f32 = jnp.bfloat16, jnp.float32
    any_spec, vm = pl.BlockSpec(memory_space=pl.ANY), pl.BlockSpec(memory_space=pltpu.VMEM)
    dma = pltpu.SemaphoreType.DMA
    held = pl.pallas_call(
        functools.partial(exchange_kernel, F, T, R, C, Q, NEAR, OUT, FINE),
        name="exchange",
        out_shape=(pltpu.VMEM((D, C), bf), pltpu.VMEM((D, C), bf), pltpu.VMEM((C, D), bf),
                   pltpu.VMEM((tok, R), f32), pltpu.VMEM((2, tok, R), bf)),
        in_specs=[any_spec] * 7,
        out_specs=(vm,) * 5,
        scratch_shapes=[
            pltpu.VMEM((1, R), f32), pltpu.VMEM((tok, D), bf), pltpu.VMEM((routes.shape[1], tok), jnp.int32),
            pltpu.VMEM((routes.shape[1], tok), f32), pltpu.VMEM((128, span), f32), pltpu.VMEM((span, 128), f32), pltpu.VMEM((R, 128), f32),
            pltpu.VMEM((3, H, C), f32), pltpu.VMEM((3, C, H), f32),
            pltpu.VMEM((2, F - 1, H, C), bf), pltpu.VMEM((F - 1, C, H), bf),
            pltpu.VMEM((tok, D), bf), pltpu.VMEM((S, D), bf), pltpu.VMEM((tok, S), bf), pltpu.VMEM((tok, S), bf),
            pltpu.VMEM((S, H // 2), f32), pltpu.VMEM((S, D), bf),
            pltpu.VMEM((S, C), f32), pltpu.VMEM((S, C), f32), pltpu.VMEM((S, C), bf),
            pltpu.VMEM((S, D), bf), pltpu.VMEM((S, D), bf), pltpu.VMEM((tok, D), bf), pltpu.VMEM((2, tok, R), bf),
            dma((2,)), dma((2, F - 1, Q)), dma((NEAR + OUT + 2 * FINE,)), dma((3,)), dma((2, F - 1, Q)), dma((NEAR + OUT + 2 * FINE,)), dma((2,)),
            dma((1,)), dma((5, 2)), dma((3,)), dma((4,)), dma((6,)),
        ],
        compiler_params=pltpu.CompilerParams(collective_id=0, has_side_effects=True, vmem_limit_bytes=42 * 1024 * 1024),
    )(gate, up, down, gain[None, :], tokens, routes.T, weight.T)
    return pl.pallas_call(
        deliver_kernel,
        name="deliver",
        out_shape=(jax.ShapeDtypeStruct((D, C), bf), jax.ShapeDtypeStruct((D, C), bf),
                   jax.ShapeDtypeStruct((C, D), bf), jax.ShapeDtypeStruct((tok, R), bf)),
        in_specs=[vm] * 5,
        out_specs=(pl.BlockSpec(memory_space=pltpu.HBM),) * 4,
        scratch_shapes=[pltpu.VMEM((tok, R), bf), dma((4,))],
        compiler_params=pltpu.CompilerParams(vmem_limit_bytes=4 * 1024 * 1024),
    )(*[pltpu.with_memory_space_constraint(x, pltpu.VMEM) for x in held])


def fits(grp_count, fs_count, pieces, gate_train):
    rows, wide = gate_train.shape[1:]
    return (grp_count == 2 and fs_count == pieces and fs_count == 4
            and wide % (fs_count * 128) == 0 and rows % 256 == 0)


def shards(tokens, routes, route_weight, norm_gain, gate_train, up_train, down_train):
    fs_count = lax.axis_size("fs")
    pieces = min(fs_count, 32)
    copies = fs_count // pieces
    if fits(lax.axis_size("grp"), fs_count, pieces, gate_train):
        gate_new, up_new, down_new, mixed = exchange(
            fs_count, lax.axis_size("tp"), gate_train[0], up_train[0], down_train[0],
            norm_gain, tokens, routes, route_weight,
        )
        return (gate_new[None], up_new[None], down_new[None], mixed)
    gain_column = norm_gain[:, None]
    gate_low = (gate_train[0] * gain_column).astype(jnp.bfloat16)
    up_low = (up_train[0] * gain_column).astype(jnp.bfloat16)
    down_low = down_train[0].astype(jnp.bfloat16)
    gate_wide = jnp.tile(gate_low, (1, copies))
    up_wide = jnp.tile(up_low, (1, copies))
    down_wide = jnp.tile(down_low, (copies, 1))
    gate_new, up_new = (
        lax.all_to_all(gate_wide, "fs", split_axis=1, concat_axis=0, tiled=True),
        lax.all_to_all(up_wide, "fs", split_axis=1, concat_axis=0, tiled=True),
    )
    down_new = lax.all_to_all(down_wide, "fs", split_axis=0, concat_axis=1, tiled=True)
    tok_float = tokens.astype(jnp.float32)
    normed = (
        tok_float * lax.rsqrt(jnp.mean(tok_float * tok_float, axis=-1, keepdims=True) + 1e-06)
    ).astype(jnp.bfloat16)
    chosen = routes.reshape(-1)
    chosen_hot = (chosen[:, None] == jnp.arange(EXPERTS, dtype=jnp.int32)[None, :]).astype(
        jnp.int32
    )
    before = jnp.cumsum(chosen_hot, axis=0) - chosen_hot
    slot_rank = jnp.sum(before * chosen_hot, axis=1)
    slot_index = (chosen * CAP + slot_rank).reshape(routes.shape)
    slot_range = jnp.arange(EXPERTS * CAP, dtype=jnp.int32)
    select_rows = jnp.any(slot_range[:, None, None] == slot_index[None, :, :], axis=-1).astype(
        jnp.bfloat16
    )
    outgoing = jnp.dot(select_rows, normed, preferred_element_type=jnp.float32).astype(jnp.bfloat16)
    outgoing = outgoing.reshape(EXPERTS, CAP, normed.shape[1])
    arrived = lax.all_to_all(outgoing, "tp", split_axis=0, concat_axis=0, tiled=True).reshape(
        EXPERTS * CAP, normed.shape[1]
    )
    slot_count = EXPERTS * CAP // copies
    copy_index = lax.axis_index("fs") // pieces
    my_rows = lax.dynamic_slice_in_dim(arrived, copy_index * slot_count, slot_count, 0)
    gated = jnp.dot(my_rows, gate_new, preferred_element_type=jnp.float32)
    lifted = jnp.dot(my_rows, up_new, preferred_element_type=jnp.float32)
    hidden = (jax.nn.silu(gated) * lifted).astype(jnp.bfloat16)
    partial_out = jnp.dot(hidden, down_new, preferred_element_type=jnp.float32)
    placed = jnp.zeros((EXPERTS * CAP, partial_out.shape[1]), jnp.float32)
    placed = lax.dynamic_update_slice_in_dim(placed, partial_out, copy_index * slot_count, 0)
    expert_out = lax.psum_scatter(placed, "fs", scatter_dimension=1, tiled=True).astype(
        jnp.bfloat16
    )
    returned = lax.all_to_all(
        expert_out.reshape(EXPERTS, CAP, expert_out.shape[1]),
        "tp",
        split_axis=0,
        concat_axis=0,
        tiled=True,
    )
    returned = returned.reshape(EXPERTS * CAP, expert_out.shape[1]).astype(jnp.float32)
    blend_weight = jnp.sum(
        jnp.where(
            slot_range[None, None, :] == slot_index[:, :, None], route_weight[:, :, None], 0.0
        ),
        axis=1,
    )
    mixed = jnp.dot(
        blend_weight, returned, precision=lax.Precision.HIGHEST, preferred_element_type=jnp.float32
    )
    return (gate_new[None], up_new[None], down_new[None], mixed.astype(jnp.bfloat16))


def solution(mesh):
    in_specs = (
        P(("grp", "tp"), None),
        P(("grp", "tp"), None),
        P(("grp", "tp"), None),
        P("fs"),
        P("tp", "fs", None),
        P("tp", "fs", None),
        P("tp", None, "fs"),
    )
    out_specs = (
        P(("grp", "tp"), None, "fs"),
        P(("grp", "tp"), None, "fs"),
        P(("grp", "tp"), "fs", None),
        P(("grp", "tp"), "fs"),
    )
    return jax.shard_map(shards, mesh=mesh, in_specs=in_specs, out_specs=out_specs, check_vma=False)
```

```python
import functools
import jax
import jax.numpy as jnp
from jax import lax
from jax.experimental import pallas as pl
from jax.experimental.pallas import tpu as pltpu
from jax.sharding import PartitionSpec as P

EXPERTS = 4
CAP = 128
MESH = pl.DeviceIdType.MESH


def exchange_kernel(F, T, R, C, Q, NEAR, OUT, FINE, gt, ut, dt, gain_at, tokens_at, routes_at, weight_at, gw, uw, dw, mown, mrecv,
                    gain, tokens, routes_t, weight_t, flat, turned, scale_at, wide, tall, sendw, sendt, normed, xs, bh, bl,
                    early, arr, gacc, uacc, hid, pbf, ret, msend, shared,
                    zs, zr, zt, ys, yr, yt, ts, ps, pr, ms, mr, loc):
    g, f, t = lax.axis_index("grp"), lax.axis_index("fs"), lax.axis_index("tp")
    H = R // 2
    wins = (gw, uw, dw)
    low = 1 - lax.div(f, 2)
    inner = lax.rem(lax.div(f + 1, 2), 2)
    near = f + 1 - 2 * lax.rem(f, 2)
    far_in = 1 + low
    far_out = 3 * low
    peers = [lax.rem(t + d, T) for d in range(1, T)]
    others = [near, far_in, far_out]
    far = [far_out, far_in]

    def pick(if_inner, if_outer):
        return inner * if_inner + (1 - inner) * if_outer

    targets = (
        (pick(far_out, near), far_in, pick(near, far_out)),
        (near, far_in, far_out),
        (near, pick(far_out, far_in), pick(far_in, far_out)),
    )
    places = (
        (pick(2, 0), pick(2, 1), pick(0, 1)),
        (0, pick(2, 1), pick(2, 1)),
    )
    items = (
        (0, pick(near, far_in), pick(0, 2)), (0, pick(far_in, near), pick(2, 0)), (1, near, 0),
        (0, far_out, 1), (1, pick(far_in, far_out), pick(2, 1)), (1, pick(far_out, far_in), pick(1, 2)),
    )

    barrier = pltpu.get_barrier_semaphore()
    for p in peers:
        pl.semaphore_signal(barrier, inc=1, device_id={"tp": p}, device_id_type=MESH)
    for p in others:
        pl.semaphore_signal(barrier, inc=1, device_id={"fs": p}, device_id_type=MESH)
    pl.semaphore_signal(barrier, inc=1, device_id={"grp": 1 - g}, device_id_type=MESH)

    def cols_of(src, half):
        return pl.ds(pl.multiple_of(src * R + half * H, H), H)

    def half_cols(half):
        return pl.ds(pl.multiple_of(half * H, H), H)

    W = H // 2
    WIDE = [(n * (H // Q), H // Q, 0, C) for n in range(Q)]
    TALL = [[(n * (C // m), C // m, 0, H) for n in range(m)] for m in (NEAR, OUT)]
    TALL.append([(n * (C // FINE), C // FINE, m * W, W) for m in range(2) for n in range(FINE)])
    ALL = len(TALL[2])
    BASE = [0, len(TALL[0]), len(TALL[0]) + len(TALL[1])]

    def part(a, src, half, piece):
        row, rows, col, cols = piece
        if a < 2:
            return wins[a].at[pl.ds(pl.multiple_of(src * R + half * H + row, rows), rows), :]
        return dw.at[pl.ds(row, rows), pl.ds(pl.multiple_of(src * R + half * H + col, W), cols)]

    def z_copy(a, k, piece, sem):
        row, rows, col, cols = piece
        held = sendw.at[a, k, pl.ds(row, rows), :] if a < 2 else sendt.at[k, pl.ds(row, rows), pl.ds(col, cols)]
        return pltpu.make_async_remote_copy(
            src_ref=held, dst_ref=part(a, f, g, piece), send_sem=zs.at[min(a, 2) // 2], recv_sem=sem,
            device_id={"fs": targets[a][k]}, device_id_type=MESH)

    def z_send(a, k, place=None):
        if a < 2:
            for q, piece in enumerate(WIDE):
                z_copy(a, k, piece, zr.at[a, places[a][k], q]).start()
        else:
            for q, piece in enumerate(TALL[place]):
                z_copy(a, k, piece, zt.at[BASE[place] + q]).start()

    def z_recv(a, src, piece, sem):
        here = part(a, src, g, piece)
        return pltpu.make_async_remote_copy(
            src_ref=here, dst_ref=here, send_sem=zs.at[min(a, 2) // 2], recv_sem=sem,
            device_id={"fs": src}, device_id_type=MESH)

    def y_copy(a, src, half, piece, sem):
        here = part(a, src, half, piece)
        return pltpu.make_async_remote_copy(
            src_ref=here, dst_ref=here, send_sem=ys.at[a], recv_sem=sem,
            device_id={"grp": 1 - g}, device_id_type=MESH)

    def sent(ref, sem):
        pltpu.make_async_remote_copy(
            src_ref=ref, dst_ref=ref, send_sem=sem, recv_sem=sem,
            device_id={"fs": near}, device_id_type=MESH).wait_send()

    def received(ref, sem):
        pltpu.make_async_remote_copy(
            src_ref=ref, dst_ref=ref, send_sem=sem, recv_sem=sem,
            device_id={"fs": near}, device_id_type=MESH).wait_recv()

    def slots(q):
        return pl.ds(pl.multiple_of(q * CAP, CAP), CAP)

    def t_copy(tgt, src):
        return pltpu.make_async_remote_copy(
            src_ref=xs.at[slots(tgt), :], dst_ref=arr.at[slots(src), :], send_sem=ts.at[0], recv_sem=ts.at[1],
            device_id={"tp": tgt}, device_id_type=MESH)

    def unit(half, chunk):
        if chunk is None:
            return half_cols(half)
        return pl.ds(pl.multiple_of(half * H + chunk * W, W), W)

    def unit_of(c, half, chunk):
        if chunk is None:
            return cols_of(c, half)
        return pl.ds(pl.multiple_of(c * R + half * H + chunk * W, W), W)

    def p_copy(c, kind, half, chunk, tgt, src):
        cols = unit_of(c, half, chunk)
        return pltpu.make_async_remote_copy(
            src_ref=pbf.at[slots(tgt), cols], dst_ref=ret.at[slots(src), cols],
            send_sem=ps.at[0], recv_sem=pr.at[kind + (chunk or 0), half],
            device_id={"tp": tgt}, device_id_type=MESH)

    def near_copy(half):
        return pltpu.make_async_remote_copy(
            src_ref=msend.at[:, cols_of(near, half)], dst_ref=mrecv.at[0, :, half_cols(half)],
            send_sem=ms.at[0], recv_sem=mr.at[0], device_id={"fs": near}, device_id_type=MESH)

    def share_copy(n, half):
        return pltpu.make_async_remote_copy(
            src_ref=msend.at[:, cols_of(far[n], half)], dst_ref=shared.at[n, :, half_cols(half)],
            send_sem=ms.at[1 + n], recv_sem=mr.at[2 + n], device_id={"fs": near}, device_id_type=MESH)

    def cross_copy(n, half, chunk):
        return pltpu.make_async_remote_copy(
            src_ref=msend.at[:, unit_of(far[n], half, chunk)], dst_ref=mrecv.at[1, :, unit(half, chunk)],
            send_sem=ms.at[1 + n], recv_sem=mr.at[1], device_id={"fs": far[n]}, device_id_type=MESH)

    tasks = [(a, k, g) for a in range(3) for k in range(3)]
    tasks += [(a, None, half) for a in range(3) for half in range(2)]

    def stage_copy(n):
        a, k, half = tasks[n]
        tgt = f if k is None else targets[a][k]
        rows, cols = half_cols(half), pl.ds(pl.multiple_of(tgt * C, C), C)
        if a < 2:
            return pltpu.make_async_copy((gt, ut)[a].at[rows, cols], wide.at[n % 3], loc.at[n % 3])
        return pltpu.make_async_copy(dt.at[cols, rows], tall.at[n % 3], loc.at[3 + n % 3])

    def cast_wide(n, begin, end):
        a, k, half = tasks[n]

        @pl.loop(begin // 32, end // 32)
        def _(m):
            rows = pl.ds(pl.multiple_of(m * 32, 32), 32)
            scale = scale_at[pl.ds(pl.multiple_of(half * H + m * 32, 32), 32), 0:1]
            value = (wide[n % 3, rows, :] * scale).astype(jnp.bfloat16)
            if k is None:
                wins[a][pl.ds(pl.multiple_of(f * R + half * H + m * 32, 32), 32), :] = value
            else:
                sendw[a, k, rows, :] = value

    def cast(n):
        a, k, half = tasks[n]
        stage_copy(n).wait()
        if a < 2:
            cast_wide(n, 0, H)
        else:
            @pl.loop(0, C // 128)
            def _(m):
                rows = pl.ds(pl.multiple_of(m * 128, 128), 128)
                value = tall[n % 3, rows, :].astype(jnp.bfloat16)
                if k is None:
                    dw[rows, cols_of(f, half)] = value
                else:
                    sendt[k, rows, :] = value
        if n + 3 < len(tasks):
            stage_copy(n + 3).start()

    def route():
        tok, slot_all = tokens.shape[0], arr.shape[0]

        @pl.loop(0, tok // 32)
        def _(m):
            rows = pl.ds(pl.multiple_of(m * 32, 32), 32)
            value = tokens[rows, :].astype(jnp.float32)
            normed[rows, :] = (
                value * lax.rsqrt(jnp.mean(value * value, axis=-1, keepdims=True) + 1e-06)
            ).astype(jnp.bfloat16)

        one, two = routes_t[0:1, :], routes_t[1:2, :]
        row = lax.broadcasted_iota(jnp.int32, (tok, tok), 0)
        col = lax.broadcasted_iota(jnp.int32, (tok, tok), 1)
        expert = lax.broadcasted_iota(jnp.int32, (16, tok), 0)
        hot = jnp.where((expert == one) | (expert == two), 1.0, 0.0).astype(jnp.bfloat16)
        before = jnp.dot(hot, jnp.where(row < col, 1.0, 0.0).astype(jnp.bfloat16), preferred_element_type=jnp.float32)
        first, second = [
            name.astype(jnp.float32) * CAP
            + jnp.sum(jnp.where(expert == name, before, 0.0), axis=0, keepdims=True)
            for name in (one, two)
        ]
        slot = lax.broadcasted_iota(jnp.int32, (slot_all, tok), 0).astype(jnp.float32)
        select = jnp.where((slot == first) | (slot == second), 1.0, 0.0).astype(jnp.bfloat16)
        for n in range(4):
            cols = pl.ds(n * (F * R // 4), F * R // 4)
            xs[:, cols] = jnp.dot(select, normed[:, cols], preferred_element_type=jnp.float32).astype(jnp.bfloat16)
        flat[...] = jnp.zeros_like(flat)
        for n, line in enumerate((first, second, weight_t[0:1, :], weight_t[1:2, :])):
            flat[n:n + 1, 0:tok] = line
        turned[...] = flat[...].T
        slot = lax.broadcasted_iota(jnp.int32, (tok, slot_all), 1).astype(jnp.float32)
        blend = jnp.where(slot == turned[0:tok, 0:1], turned[0:tok, 2:3], 0.0) + jnp.where(
            slot == turned[0:tok, 1:2], turned[0:tok, 3:4], 0.0)
        high = blend.astype(jnp.bfloat16)
        bh[...] = high
        bl[...] = (blend - high.astype(jnp.float32)).astype(jnp.bfloat16)

    idle = (ps.at[0], ms.at[0], ms.at[1], ms.at[2])

    def first_copy(q):
        rows = pl.ds(pl.multiple_of(g * H + q * (H // Q), H // Q), H // Q)
        cols = pl.ds(pl.multiple_of(targets[0][0] * C, C), C)
        return pltpu.make_async_copy(gt.at[rows, cols], wide.at[0, pl.ds(q * (H // Q), H // Q), :], idle[q])

    small = [pltpu.make_async_copy(a, b, c) for a, b, c in (
        (gain_at, gain, ts.at[0]), (tokens_at, tokens, loc.at[3]),
        (routes_at, routes_t, loc.at[4]), (weight_at, weight_t, loc.at[5]))]
    small[0].start()
    for q in range(Q):
        first_copy(q).start()
    for n in range(1, 3):
        stage_copy(n).start()
    for copy in small[1:]:
        copy.start()
    small[0].wait()
    for n in range(R // 128):
        piece = pl.ds(n * 128, 128)
        scale_at[piece, :] = jnp.broadcast_to(gain[0:1, piece], (128, 128)).T
    for q in range(Q):
        first_copy(q).wait()
        cast_wide(0, q * (H // Q), (q + 1) * (H // Q))
        if q == 0:
            pl.semaphore_wait(barrier, len(peers) + len(others) + 1)
        else:
            z_copy(0, 0, WIDE[q - 1], zr.at[0, places[0][0], q - 1]).start()
    stage_copy(3).start()
    for n in range(1, 9):
        if n == 3:
            for copy in small[1:]:
                copy.wait()
        cast(n)
        a, k = tasks[n - 1][:2]
        if n == 1:
            z_copy(0, 0, WIDE[Q - 1], zr.at[0, places[0][0], Q - 1]).start()
        elif n < 8:
            @pl.when(inner == 1)
            def _():
                z_send(a, k, 0)
        else:
            @pl.when(inner == 1)
            def _():
                z_send(2, 1, 2)

            @pl.when(inner == 0)
            def _():
                for pair in ((1, 0), (2, 0), (0, 1), (0, 2), (1, 1), (1, 2)):
                    z_send(*pair, 0)
    route()

    @pl.when(inner == 1)
    def _():
        z_send(2, 2, 2)

    for n in range(9, len(tasks)):
        cast(n)
        if n == 9:
            for p in peers:
                t_copy(p, t).start()
    arr[slots(t), :] = xs[slots(t), :]

    rows_all = arr.shape[0]
    M = min(256, rows_all)

    def multiply(a, src, first):
        acc = (gacc, uacc)[a]
        deep = pl.ds(pl.multiple_of(src * R, R), R)

        @pl.loop(0, rows_all // M)
        def _(m):
            rows = pl.ds(pl.multiple_of(m * M, M), M)
            value = jnp.dot(arr[rows, deep], wins[a][deep, :], preferred_element_type=jnp.float32)
            if first:
                acc[rows, :] = value
            else:
                acc[rows, :] += value

    def activate():
        @pl.loop(0, rows_all // 64)
        def _(m):
            rows = pl.ds(pl.multiple_of(m * 64, 64), 64)
            v = gacc[rows, :]
            hid[rows, :] = (v / (1.0 + jnp.exp(-v)) * uacc[rows, :]).astype(jnp.bfloat16)

    def partial_out(c, kind, half, chunk=None):
        cols = unit_of(c, half, chunk)

        @pl.loop(0, rows_all // M)
        def _(m):
            rows = pl.ds(pl.multiple_of(m * M, M), M)
            pbf[rows, cols] = jnp.dot(hid[rows, :], dw[:, cols], preferred_element_type=jnp.float32).astype(jnp.bfloat16)

        for p in peers:
            p_copy(c, kind, half, chunk, p, t).start()
        ret[slots(t), cols] = pbf[slots(t), cols]

    def spread(c, kind, half, chunk):
        cols = unit_of(c, half, chunk)
        for p in peers:
            p_copy(c, kind, half, chunk, p, t).start()
        ret[slots(t), cols] = pbf[slots(t), cols]

    def partial_early(half, cut):
        early[...] = jnp.dot(hid[:, 0:cut], dw[0:cut, unit_of(far_in, half, 1)], preferred_element_type=jnp.float32)

    def partial_late(half, cut):
        cols = unit_of(far_in, half, 1)
        value = early[...] + jnp.dot(hid[:, cut:C], dw[cut:C, cols], preferred_element_type=jnp.float32)
        pbf[:, cols] = value.astype(jnp.bfloat16)
        spread(far_in, 3, half, 1)

    def mix(c, kind, half, chunk=None):
        cols = unit_of(c, half, chunk)
        received(ret.at[pl.ds(0, len(peers) * CAP), cols], pr.at[kind + (chunk or 0), half])
        return jnp.dot(bh[...], ret[:, cols], preferred_element_type=jnp.float32) + jnp.dot(
            bl[...], ret[:, cols], preferred_element_type=jnp.float32)

    def mix_own(half):
        mown[:, half_cols(half)] = mix(f, 0, half)

    def mix_near(half):
        msend[:, cols_of(near, half)] = mix(near, 1, half).astype(jnp.bfloat16)
        near_copy(half).start()

    def join(n, half, chunk=None):
        cols = unit_of(far[n], half, chunk)
        both = mix(far[n], 2 + n, half, chunk) + shared[n, :, unit(half, chunk)].astype(jnp.float32)
        msend[:, cols] = both.astype(jnp.bfloat16)
        cross_copy(n, half, chunk).start()

    def share(n, half):
        msend[:, cols_of(far[n], half)] = mix(far[n], 2 + n, half).astype(jnp.bfloat16)
        share_copy(n, half).start()

    def stream(a, place):
        if a < 2:
            return [(piece, zr.at[a, place, q], yr.at[a, place]) for q, piece in enumerate(WIDE)]
        last = len(TALL[place]) - 1
        return [(piece, zt.at[BASE[place] + q], yt.at[place + (q >= FINE) + (q == last) if place == 2 else place])
                for q, piece in enumerate(TALL[place])]

    def forward(a, src, place, begin, end):
        for piece, z, y in stream(a, place)[begin:end]:
            z_recv(a, src, piece, z).wait_recv()
            y_copy(a, src, g, piece, y).start()

    def landed(a, src, place):
        whole = (0, H, 0, C) if a < 2 else (0, C, 0, H)
        y_copy(a, src, 1 - g, whole, yr.at[a, place] if a < 2 else yt.at[place]).wait_recv()

    def landed_in(*groups):
        rows = C - C // FINE
        for n in groups:
            piece = ((0, C, 0, W), (0, rows, W, W), (rows, C - rows, W, W))[n]
            y_copy(2, far_in, 1 - g, piece, yt.at[2 + n]).wait_recv()

    def settle(a, src, place):
        landed(a, src, place)
        multiply(a, src, False)

    half_way = Q // 2
    forward(*items[0], 0, Q)
    forward(*items[1], 0, Q)
    received(xs.at[pl.ds(0, len(peers) * CAP), :], ts.at[1])
    for a in (0, 1):
        multiply(a, f, True)
    for n in range(2, 6):
        forward(*items[n], 0, half_way)
        settle(*items[n - 2])
        forward(*items[n], half_way, Q)
        if n == 3:
            forward(2, near, 0, 0, NEAR)
    settle(*items[4])

    @pl.when(inner == 0)
    def _():
        z_send(2, 2, 1)
        z_send(2, 1, 1)

    settle(*items[5])
    activate()
    partial_out(f, 0, 0)
    partial_out(f, 0, 1)
    partial_out(near, 1, g)
    landed(2, near, 0)
    partial_out(near, 1, 1 - g)
    mix_own(0)
    mix_own(1)
    mix_near(g)
    forward(2, far_out, 1, 0, 1)
    mix_near(1 - g)
    forward(2, far_out, 1, 1, OUT)
    partial_out(far_out, 2, g)

    def forward_in(begin, end):
        forward(2, far_in, 2, begin, end)

    @pl.when(inner == 0)
    def _():
        forward_in(0, FINE)
        landed(2, far_out, 1)
        partial_out(far_out, 2, 1 - g)
        forward_in(FINE, ALL)
        share(0, g)
        share(0, 1 - g)
        partial_out(far_in, 3, g)
        landed_in(0, 1, 2)
        partial_out(far_in, 3, 1 - g)
        share(1, g)
        share(1, 1 - g)

    @pl.when(inner == 1)
    def _():
        landed(2, far_out, 1)
        partial_out(far_out, 2, 1 - g)
        forward_in(0, FINE)
        partial_out(far_in, 3, g, 0)
        forward_in(FINE, FINE + FINE // 2)
        landed_in(0)
        partial_out(far_in, 3, 1 - g, 0)
        forward_in(FINE + FINE // 2, ALL - 1)
        received(shared.at[0], mr.at[2])
        join(0, g)
        join(0, 1 - g)
        forward_in(ALL - 1, ALL)
        partial_out(far_in, 3, g, 1)
        received(shared.at[1], mr.at[3])
        join(1, g, 0)
        join(1, 1 - g, 0)
        cut = (ALL - FINE - 1) * C // FINE // 128 * 128
        landed_in(1)
        partial_early(1 - g, cut)
        landed_in(2)
        partial_late(1 - g, cut)
        join(1, g, 1)
        join(1, 1 - g, 1)

    sent(xs.at[pl.ds(0, len(peers) * CAP), :], ts.at[0])
    sent(sendw, zs.at[0])
    sent(sendt, zs.at[1])
    for a in range(3):
        sent(sendw.at[a] if a < 2 else sendt, ys.at[a])
    sent(pbf.at[pl.ds(0, len(peers) * CAP), :], ps.at[0])
    received(mrecv.at[0], mr.at[0])
    received(mrecv.at[1], mr.at[1])
    for n in range(3):
        sent(msend.at[:, pl.ds(0, R)], ms.at[n])


def deliver_kernel(gw, uw, dw, mown, mrecv, go, uo, do, mo, total, sems):
    copies = [pltpu.make_async_copy(a, b, sems.at[n]) for n, (a, b) in enumerate(((gw, go), (uw, uo), (dw, do)))]
    for copy in copies:
        copy.start()
    value = mown[...]
    for n in range(mrecv.shape[0]):
        value = value + mrecv[n].astype(jnp.float32)
    total[...] = value.astype(jnp.bfloat16)
    last = pltpu.make_async_copy(total, mo, sems.at[len(copies)])
    last.start()
    for copy in copies + [last]:
        copy.wait()


def exchange(F, T, gate, up, down, gain, tokens, routes, weight):
    span = -(-tokens.shape[0] // 128) * 128
    R, FF = gate.shape
    C, D, H = FF // F, F * R, R // 2
    Q, NEAR, OUT, FINE = 4, 1, 2, 8
    tok, S = tokens.shape[0], EXPERTS * CAP
    bf, f32 = jnp.bfloat16, jnp.float32
    any_spec, vm = pl.BlockSpec(memory_space=pl.ANY), pl.BlockSpec(memory_space=pltpu.VMEM)
    dma = pltpu.SemaphoreType.DMA
    held = pl.pallas_call(
        functools.partial(exchange_kernel, F, T, R, C, Q, NEAR, OUT, FINE),
        name="exchange",
        out_shape=(pltpu.VMEM((D, C), bf), pltpu.VMEM((D, C), bf), pltpu.VMEM((C, D), bf),
                   pltpu.VMEM((tok, R), f32), pltpu.VMEM((2, tok, R), bf)),
        in_specs=[any_spec] * 7,
        out_specs=(vm,) * 5,
        scratch_shapes=[
            pltpu.VMEM((1, R), f32), pltpu.VMEM((tok, D), bf), pltpu.VMEM((routes.shape[1], tok), jnp.int32),
            pltpu.VMEM((routes.shape[1], tok), f32), pltpu.VMEM((128, span), f32), pltpu.VMEM((span, 128), f32), pltpu.VMEM((R, 128), f32),
            pltpu.VMEM((3, H, C), f32), pltpu.VMEM((3, C, H), f32),
            pltpu.VMEM((2, F - 1, H, C), bf), pltpu.VMEM((F - 1, C, H), bf),
            pltpu.VMEM((tok, D), bf), pltpu.VMEM((S, D), bf), pltpu.VMEM((tok, S), bf), pltpu.VMEM((tok, S), bf),
            pltpu.VMEM((S, H // 2), f32), pltpu.VMEM((S, D), bf),
            pltpu.VMEM((S, C), f32), pltpu.VMEM((S, C), f32), pltpu.VMEM((S, C), bf),
            pltpu.VMEM((S, D), bf), pltpu.VMEM((S, D), bf), pltpu.VMEM((tok, D), bf), pltpu.VMEM((2, tok, R), bf),
            dma((2,)), dma((2, F - 1, Q)), dma((NEAR + OUT + 2 * FINE,)), dma((3,)), dma((2, F - 1)), dma((5,)), dma((2,)),
            dma((1,)), dma((5, 2)), dma((3,)), dma((4,)), dma((6,)),
        ],
        compiler_params=pltpu.CompilerParams(collective_id=0, has_side_effects=True, vmem_limit_bytes=42 * 1024 * 1024),
    )(gate, up, down, gain[None, :], tokens, routes.T, weight.T)
    return pl.pallas_call(
        deliver_kernel,
        name="deliver",
        out_shape=(jax.ShapeDtypeStruct((D, C), bf), jax.ShapeDtypeStruct((D, C), bf),
                   jax.ShapeDtypeStruct((C, D), bf), jax.ShapeDtypeStruct((tok, R), bf)),
        in_specs=[vm] * 5,
        out_specs=(pl.BlockSpec(memory_space=pltpu.HBM),) * 4,
        scratch_shapes=[pltpu.VMEM((tok, R), bf), dma((4,))],
        compiler_params=pltpu.CompilerParams(vmem_limit_bytes=4 * 1024 * 1024),
    )(*[pltpu.with_memory_space_constraint(x, pltpu.VMEM) for x in held])


def fits(grp_count, fs_count, pieces, gate_train):
    rows, wide = gate_train.shape[1:]
    return (grp_count == 2 and fs_count == pieces and fs_count == 4
            and wide % (fs_count * 128) == 0 and rows % 256 == 0)


def shards(tokens, routes, route_weight, norm_gain, gate_train, up_train, down_train):
    fs_count = lax.axis_size("fs")
    pieces = min(fs_count, 32)
    copies = fs_count // pieces
    if fits(lax.axis_size("grp"), fs_count, pieces, gate_train):
        gate_new, up_new, down_new, mixed = exchange(
            fs_count, lax.axis_size("tp"), gate_train[0], up_train[0], down_train[0],
            norm_gain, tokens, routes, route_weight,
        )
        return (gate_new[None], up_new[None], down_new[None], mixed)
    gain_column = norm_gain[:, None]
    gate_low = (gate_train[0] * gain_column).astype(jnp.bfloat16)
    up_low = (up_train[0] * gain_column).astype(jnp.bfloat16)
    down_low = down_train[0].astype(jnp.bfloat16)
    gate_wide = jnp.tile(gate_low, (1, copies))
    up_wide = jnp.tile(up_low, (1, copies))
    down_wide = jnp.tile(down_low, (copies, 1))
    gate_new, up_new = (
        lax.all_to_all(gate_wide, "fs", split_axis=1, concat_axis=0, tiled=True),
        lax.all_to_all(up_wide, "fs", split_axis=1, concat_axis=0, tiled=True),
    )
    down_new = lax.all_to_all(down_wide, "fs", split_axis=0, concat_axis=1, tiled=True)
    tok_float = tokens.astype(jnp.float32)
    normed = (
        tok_float * lax.rsqrt(jnp.mean(tok_float * tok_float, axis=-1, keepdims=True) + 1e-06)
    ).astype(jnp.bfloat16)
    chosen = routes.reshape(-1)
    chosen_hot = (chosen[:, None] == jnp.arange(EXPERTS, dtype=jnp.int32)[None, :]).astype(
        jnp.int32
    )
    before = jnp.cumsum(chosen_hot, axis=0) - chosen_hot
    slot_rank = jnp.sum(before * chosen_hot, axis=1)
    slot_index = (chosen * CAP + slot_rank).reshape(routes.shape)
    slot_range = jnp.arange(EXPERTS * CAP, dtype=jnp.int32)
    select_rows = jnp.any(slot_range[:, None, None] == slot_index[None, :, :], axis=-1).astype(
        jnp.bfloat16
    )
    outgoing = jnp.dot(select_rows, normed, preferred_element_type=jnp.float32).astype(jnp.bfloat16)
    outgoing = outgoing.reshape(EXPERTS, CAP, normed.shape[1])
    arrived = lax.all_to_all(outgoing, "tp", split_axis=0, concat_axis=0, tiled=True).reshape(
        EXPERTS * CAP, normed.shape[1]
    )
    slot_count = EXPERTS * CAP // copies
    copy_index = lax.axis_index("fs") // pieces
    my_rows = lax.dynamic_slice_in_dim(arrived, copy_index * slot_count, slot_count, 0)
    gated = jnp.dot(my_rows, gate_new, preferred_element_type=jnp.float32)
    lifted = jnp.dot(my_rows, up_new, preferred_element_type=jnp.float32)
    hidden = (jax.nn.silu(gated) * lifted).astype(jnp.bfloat16)
    partial_out = jnp.dot(hidden, down_new, preferred_element_type=jnp.float32)
    placed = jnp.zeros((EXPERTS * CAP, partial_out.shape[1]), jnp.float32)
    placed = lax.dynamic_update_slice_in_dim(placed, partial_out, copy_index * slot_count, 0)
    expert_out = lax.psum_scatter(placed, "fs", scatter_dimension=1, tiled=True).astype(
        jnp.bfloat16
    )
    returned = lax.all_to_all(
        expert_out.reshape(EXPERTS, CAP, expert_out.shape[1]),
        "tp",
        split_axis=0,
        concat_axis=0,
        tiled=True,
    )
    returned = returned.reshape(EXPERTS * CAP, expert_out.shape[1]).astype(jnp.float32)
    blend_weight = jnp.sum(
        jnp.where(
            slot_range[None, None, :] == slot_index[:, :, None], route_weight[:, :, None], 0.0
        ),
        axis=1,
    )
    mixed = jnp.dot(
        blend_weight, returned, precision=lax.Precision.HIGHEST, preferred_element_type=jnp.float32
    )
    return (gate_new[None], up_new[None], down_new[None], mixed.astype(jnp.bfloat16))


def solution(mesh):
    in_specs = (
        P(("grp", "tp"), None),
        P(("grp", "tp"), None),
        P(("grp", "tp"), None),
        P("fs"),
        P("tp", "fs", None),
        P("tp", "fs", None),
        P("tp", None, "fs"),
    )
    out_specs = (
        P(("grp", "tp"), None, "fs"),
        P(("grp", "tp"), None, "fs"),
        P(("grp", "tp"), "fs", None),
        P(("grp", "tp"), "fs"),
    )
    return jax.shard_map(shards, mesh=mesh, in_specs=in_specs, out_specs=out_specs, check_vma=False)
```

```python
import functools
import jax
import jax.numpy as jnp
from jax import lax
from jax.experimental import pallas as pl
from jax.experimental.pallas import tpu as pltpu
from jax.sharding import PartitionSpec as P

EXPERTS = 4
CAP = 128
MESH = pl.DeviceIdType.MESH


def exchange_kernel(F, T, R, C, Q, NEAR, OUT, FINE, gt, ut, dt, gain_at, tokens_at, routes_at, weight_at, gw, uw, dw, mown, mrecv,
                    gain, tokens, routes_t, weight_t, flat, turned, scale_at, wide, tall, sendw, sendt, normed, xs, bh, bl,
                    early, arr, gacc, uacc, hid, pbf, ret, msend, shared,
                    zs, zr, zt, ys, yr, yt, ts, ps, pr, ms, mr, loc):
    g, f, t = lax.axis_index("grp"), lax.axis_index("fs"), lax.axis_index("tp")
    H = R // 2
    wins = (gw, uw, dw)
    low = 1 - lax.div(f, 2)
    inner = lax.rem(lax.div(f + 1, 2), 2)
    near = f + 1 - 2 * lax.rem(f, 2)
    far_in = 1 + low
    far_out = 3 * low
    peers = [lax.rem(t + d, T) for d in range(1, T)]
    others = [near, far_in, far_out]
    far = [far_out, far_in]

    def pick(if_inner, if_outer):
        return inner * if_inner + (1 - inner) * if_outer

    targets = (
        (pick(far_out, near), far_in, pick(near, far_out)),
        (near, far_in, far_out),
        (near, pick(far_out, far_in), pick(far_in, far_out)),
    )
    places = (
        (pick(2, 0), pick(2, 1), pick(0, 1)),
        (0, pick(2, 1), pick(2, 1)),
    )
    items = (
        (0, pick(near, far_in), pick(0, 2)), (0, pick(far_in, near), pick(2, 0)), (1, near, 0),
        (0, far_out, 1), (1, pick(far_in, far_out), pick(2, 1)), (1, pick(far_out, far_in), pick(1, 2)),
    )

    barrier = pltpu.get_barrier_semaphore()
    for p in peers:
        pl.semaphore_signal(barrier, inc=1, device_id={"tp": p}, device_id_type=MESH)
    for p in others:
        pl.semaphore_signal(barrier, inc=1, device_id={"fs": p}, device_id_type=MESH)
    pl.semaphore_signal(barrier, inc=1, device_id={"grp": 1 - g}, device_id_type=MESH)

    def cols_of(src, half):
        return pl.ds(pl.multiple_of(src * R + half * H, H), H)

    def half_cols(half):
        return pl.ds(pl.multiple_of(half * H, H), H)

    W = H // 2
    WIDE = [(n * (H // Q), H // Q, 0, C) for n in range(Q)]
    TALL = [[(n * (C // m), C // m, 0, H) for n in range(m)] for m in (NEAR, OUT)]
    TALL.append([(n * (C // FINE), C // FINE, m * W, W) for m in range(2) for n in range(FINE)])
    ALL = len(TALL[2])
    BASE = [0, len(TALL[0]), len(TALL[0]) + len(TALL[1])]

    def part(a, src, half, piece):
        row, rows, col, cols = piece
        if a < 2:
            return wins[a].at[pl.ds(pl.multiple_of(src * R + half * H + row, rows), rows), :]
        return dw.at[pl.ds(row, rows), pl.ds(pl.multiple_of(src * R + half * H + col, W), cols)]

    def z_copy(a, k, piece, sem):
        row, rows, col, cols = piece
        held = sendw.at[a, k, pl.ds(row, rows), :] if a < 2 else sendt.at[k, pl.ds(row, rows), pl.ds(col, cols)]
        return pltpu.make_async_remote_copy(
            src_ref=held, dst_ref=part(a, f, g, piece), send_sem=zs.at[min(a, 2) // 2], recv_sem=sem,
            device_id={"fs": targets[a][k]}, device_id_type=MESH)

    def z_send(a, k, place=None):
        if a < 2:
            for q, piece in enumerate(WIDE):
                z_copy(a, k, piece, zr.at[a, places[a][k], q]).start()
        else:
            for q, piece in enumerate(TALL[place]):
                z_copy(a, k, piece, zt.at[BASE[place] + q]).start()

    def z_recv(a, src, piece, sem):
        here = part(a, src, g, piece)
        return pltpu.make_async_remote_copy(
            src_ref=here, dst_ref=here, send_sem=zs.at[min(a, 2) // 2], recv_sem=sem,
            device_id={"fs": src}, device_id_type=MESH)

    def y_copy(a, src, half, piece, sem):
        here = part(a, src, half, piece)
        return pltpu.make_async_remote_copy(
            src_ref=here, dst_ref=here, send_sem=ys.at[a], recv_sem=sem,
            device_id={"grp": 1 - g}, device_id_type=MESH)

    def sent(ref, sem):
        pltpu.make_async_remote_copy(
            src_ref=ref, dst_ref=ref, send_sem=sem, recv_sem=sem,
            device_id={"fs": near}, device_id_type=MESH).wait_send()

    def received(ref, sem):
        pltpu.make_async_remote_copy(
            src_ref=ref, dst_ref=ref, send_sem=sem, recv_sem=sem,
            device_id={"fs": near}, device_id_type=MESH).wait_recv()

    def slots(q):
        return pl.ds(pl.multiple_of(q * CAP, CAP), CAP)

    def t_copy(tgt, src):
        return pltpu.make_async_remote_copy(
            src_ref=xs.at[slots(tgt), :], dst_ref=arr.at[slots(src), :], send_sem=ts.at[0], recv_sem=ts.at[1],
            device_id={"tp": tgt}, device_id_type=MESH)

    def unit(half, chunk):
        if chunk is None:
            return half_cols(half)
        return pl.ds(pl.multiple_of(half * H + chunk * W, W), W)

    def unit_of(c, half, chunk):
        if chunk is None:
            return cols_of(c, half)
        return pl.ds(pl.multiple_of(c * R + half * H + chunk * W, W), W)

    def p_copy(c, kind, half, chunk, tgt, src):
        cols = unit_of(c, half, chunk)
        return pltpu.make_async_remote_copy(
            src_ref=pbf.at[slots(tgt), cols], dst_ref=ret.at[slots(src), cols],
            send_sem=ps.at[0], recv_sem=pr.at[kind + (chunk or 0), half],
            device_id={"tp": tgt}, device_id_type=MESH)

    def near_copy(half):
        return pltpu.make_async_remote_copy(
            src_ref=msend.at[:, cols_of(near, half)], dst_ref=mrecv.at[0, :, half_cols(half)],
            send_sem=ms.at[0], recv_sem=mr.at[0], device_id={"fs": near}, device_id_type=MESH)

    def share_copy(n, half):
        return pltpu.make_async_remote_copy(
            src_ref=msend.at[:, cols_of(far[n], half)], dst_ref=shared.at[n, :, half_cols(half)],
            send_sem=ms.at[1 + n], recv_sem=mr.at[2 + n], device_id={"fs": near}, device_id_type=MESH)

    def cross_copy(n, half, chunk):
        return pltpu.make_async_remote_copy(
            src_ref=msend.at[:, unit_of(far[n], half, chunk)], dst_ref=mrecv.at[1, :, unit(half, chunk)],
            send_sem=ms.at[1 + n], recv_sem=mr.at[1], device_id={"fs": far[n]}, device_id_type=MESH)

    tasks = [(a, k, g) for a in range(3) for k in range(3)]
    tasks += [(a, None, half) for a in range(3) for half in range(2)]

    def stage_copy(n):
        a, k, half = tasks[n]
        tgt = f if k is None else targets[a][k]
        rows, cols = half_cols(half), pl.ds(pl.multiple_of(tgt * C, C), C)
        if a < 2:
            return pltpu.make_async_copy((gt, ut)[a].at[rows, cols], wide.at[n % 3], loc.at[n % 3])
        return pltpu.make_async_copy(dt.at[cols, rows], tall.at[n % 3], loc.at[3 + n % 3])

    def cast_wide(n, begin, end):
        a, k, half = tasks[n]

        @pl.loop(begin // 32, end // 32)
        def _(m):
            rows = pl.ds(pl.multiple_of(m * 32, 32), 32)
            scale = scale_at[pl.ds(pl.multiple_of(half * H + m * 32, 32), 32), 0:1]
            value = (wide[n % 3, rows, :] * scale).astype(jnp.bfloat16)
            if k is None:
                wins[a][pl.ds(pl.multiple_of(f * R + half * H + m * 32, 32), 32), :] = value
            else:
                sendw[a, k, rows, :] = value

    def cast(n):
        a, k, half = tasks[n]
        stage_copy(n).wait()
        if a < 2:
            cast_wide(n, 0, H)
        else:
            @pl.loop(0, C // 128)
            def _(m):
                rows = pl.ds(pl.multiple_of(m * 128, 128), 128)
                value = tall[n % 3, rows, :].astype(jnp.bfloat16)
                if k is None:
                    dw[rows, cols_of(f, half)] = value
                else:
                    sendt[k, rows, :] = value
        if n + 3 < len(tasks):
            stage_copy(n + 3).start()

    def route():
        tok, slot_all = tokens.shape[0], arr.shape[0]

        @pl.loop(0, tok // 32)
        def _(m):
            rows = pl.ds(pl.multiple_of(m * 32, 32), 32)
            value = tokens[rows, :].astype(jnp.float32)
            normed[rows, :] = (
                value * lax.rsqrt(jnp.mean(value * value, axis=-1, keepdims=True) + 1e-06)
            ).astype(jnp.bfloat16)

        one, two = routes_t[0:1, :], routes_t[1:2, :]
        row = lax.broadcasted_iota(jnp.int32, (tok, tok), 0)
        col = lax.broadcasted_iota(jnp.int32, (tok, tok), 1)
        expert = lax.broadcasted_iota(jnp.int32, (16, tok), 0)
        hot = jnp.where((expert == one) | (expert == two), 1.0, 0.0).astype(jnp.bfloat16)
        before = jnp.dot(hot, jnp.where(row < col, 1.0, 0.0).astype(jnp.bfloat16), preferred_element_type=jnp.float32)
        first, second = [
            name.astype(jnp.float32) * CAP
            + jnp.sum(jnp.where(expert == name, before, 0.0), axis=0, keepdims=True)
            for name in (one, two)
        ]
        slot = lax.broadcasted_iota(jnp.int32, (slot_all, tok), 0).astype(jnp.float32)
        select = jnp.where((slot == first) | (slot == second), 1.0, 0.0).astype(jnp.bfloat16)
        for n in range(4):
            cols = pl.ds(n * (F * R // 4), F * R // 4)
            xs[:, cols] = jnp.dot(select, normed[:, cols], preferred_element_type=jnp.float32).astype(jnp.bfloat16)
        flat[...] = jnp.zeros_like(flat)
        for n, line in enumerate((first, second, weight_t[0:1, :], weight_t[1:2, :])):
            flat[n:n + 1, 0:tok] = line
        turned[...] = flat[...].T
        slot = lax.broadcasted_iota(jnp.int32, (tok, slot_all), 1).astype(jnp.float32)
        blend = jnp.where(slot == turned[0:tok, 0:1], turned[0:tok, 2:3], 0.0) + jnp.where(
            slot == turned[0:tok, 1:2], turned[0:tok, 3:4], 0.0)
        high = blend.astype(jnp.bfloat16)
        bh[...] = high
        bl[...] = (blend - high.astype(jnp.float32)).astype(jnp.bfloat16)

    idle = (ps.at[0], ms.at[0], ms.at[1], ms.at[2])

    def first_copy(q):
        rows = pl.ds(pl.multiple_of(g * H + q * (H // Q), H // Q), H // Q)
        cols = pl.ds(pl.multiple_of(targets[0][0] * C, C), C)
        return pltpu.make_async_copy(gt.at[rows, cols], wide.at[0, pl.ds(q * (H // Q), H // Q), :], idle[q])

    small = [pltpu.make_async_copy(a, b, c) for a, b, c in (
        (gain_at, gain, ts.at[0]), (tokens_at, tokens, loc.at[3]),
        (routes_at, routes_t, loc.at[4]), (weight_at, weight_t, loc.at[5]))]
    small[0].start()
    for q in range(Q):
        first_copy(q).start()
    for n in range(1, 3):
        stage_copy(n).start()
    for copy in small[1:]:
        copy.start()
    small[0].wait()
    for n in range(R // 128):
        piece = pl.ds(n * 128, 128)
        scale_at[piece, :] = jnp.broadcast_to(gain[0:1, piece], (128, 128)).T
    for q in range(Q):
        first_copy(q).wait()
        cast_wide(0, q * (H // Q), (q + 1) * (H // Q))
        if q == 0:
            pl.semaphore_wait(barrier, len(peers) + len(others) + 1)
        else:
            z_copy(0, 0, WIDE[q - 1], zr.at[0, places[0][0], q - 1]).start()
    stage_copy(3).start()
    for n in range(1, 9):
        if n == 3:
            for copy in small[1:]:
                copy.wait()
        cast(n)
        a, k = tasks[n - 1][:2]
        if n == 1:
            z_copy(0, 0, WIDE[Q - 1], zr.at[0, places[0][0], Q - 1]).start()
        elif n < 8:
            @pl.when(inner == 1)
            def _():
                z_send(a, k, 0)
        else:
            @pl.when(inner == 1)
            def _():
                z_send(2, 1, 2)

            @pl.when(inner == 0)
            def _():
                for pair in ((1, 0), (2, 0), (0, 1), (0, 2), (1, 1), (1, 2)):
                    z_send(*pair, 0)
    route()

    @pl.when(inner == 1)
    def _():
        z_send(2, 2, 2)

    for n in range(9, len(tasks)):
        cast(n)
        if n == 9:
            for p in peers:
                t_copy(p, t).start()
    arr[slots(t), :] = xs[slots(t), :]

    rows_all = arr.shape[0]
    M = min(256, rows_all)

    def multiply(a, src, first):
        acc = (gacc, uacc)[a]
        deep = pl.ds(pl.multiple_of(src * R, R), R)

        @pl.loop(0, rows_all // M)
        def _(m):
            rows = pl.ds(pl.multiple_of(m * M, M), M)
            value = jnp.dot(arr[rows, deep], wins[a][deep, :], preferred_element_type=jnp.float32)
            if first:
                acc[rows, :] = value
            else:
                acc[rows, :] += value

    def activate():
        @pl.loop(0, rows_all // 64)
        def _(m):
            rows = pl.ds(pl.multiple_of(m * 64, 64), 64)
            v = gacc[rows, :]
            hid[rows, :] = (v / (1.0 + jnp.exp(-v)) * uacc[rows, :]).astype(jnp.bfloat16)

    def partial_out(c, kind, half, chunk=None):
        cols = unit_of(c, half, chunk)

        @pl.loop(0, rows_all // M)
        def _(m):
            rows = pl.ds(pl.multiple_of(m * M, M), M)
            pbf[rows, cols] = jnp.dot(hid[rows, :], dw[:, cols], preferred_element_type=jnp.float32).astype(jnp.bfloat16)

        for p in peers:
            p_copy(c, kind, half, chunk, p, t).start()
        ret[slots(t), cols] = pbf[slots(t), cols]

    def spread(c, kind, half, chunk):
        cols = unit_of(c, half, chunk)
        for p in peers:
            p_copy(c, kind, half, chunk, p, t).start()
        ret[slots(t), cols] = pbf[slots(t), cols]

    def partial_early(half, cut):
        early[...] = jnp.dot(hid[:, 0:cut], dw[0:cut, unit_of(far_in, half, 1)], preferred_element_type=jnp.float32)

    def partial_late(half, cut):
        cols = unit_of(far_in, half, 1)
        value = early[...] + jnp.dot(hid[:, cut:C], dw[cut:C, cols], preferred_element_type=jnp.float32)
        pbf[:, cols] = value.astype(jnp.bfloat16)
        spread(far_in, 3, half, 1)

    def mix(c, kind, half, chunk=None):
        cols = unit_of(c, half, chunk)
        received(ret.at[pl.ds(0, len(peers) * CAP), cols], pr.at[kind + (chunk or 0), half])
        return jnp.dot(bh[...], ret[:, cols], preferred_element_type=jnp.float32) + jnp.dot(
            bl[...], ret[:, cols], preferred_element_type=jnp.float32)

    def mix_own(half):
        mown[:, half_cols(half)] = mix(f, 0, half)

    def mix_near(half):
        msend[:, cols_of(near, half)] = mix(near, 1, half).astype(jnp.bfloat16)
        near_copy(half).start()

    def join(n, half, chunk=None):
        cols = unit_of(far[n], half, chunk)
        both = mix(far[n], 2 + n, half, chunk) + shared[n, :, unit(half, chunk)].astype(jnp.float32)
        msend[:, cols] = both.astype(jnp.bfloat16)
        cross_copy(n, half, chunk).start()

    def share(n, half):
        msend[:, cols_of(far[n], half)] = mix(far[n], 2 + n, half).astype(jnp.bfloat16)
        share_copy(n, half).start()

    def stream(a, place):
        if a < 2:
            return [(piece, zr.at[a, place, q], yr.at[a, place]) for q, piece in enumerate(WIDE)]
        last = len(TALL[place]) - 1
        return [(piece, zt.at[BASE[place] + q], yt.at[place + (q >= FINE) + (q == last) if place == 2 else place])
                for q, piece in enumerate(TALL[place])]

    def forward(a, src, place, begin, end):
        for piece, z, y in stream(a, place)[begin:end]:
            z_recv(a, src, piece, z).wait_recv()
            y_copy(a, src, g, piece, y).start()

    def landed(a, src, place):
        whole = (0, H, 0, C) if a < 2 else (0, C, 0, H)
        y_copy(a, src, 1 - g, whole, yr.at[a, place] if a < 2 else yt.at[place]).wait_recv()

    def landed_in(*groups):
        rows = C - C // FINE
        for n in groups:
            piece = ((0, C, 0, W), (0, rows, W, W), (rows, C - rows, W, W))[n]
            y_copy(2, far_in, 1 - g, piece, yt.at[2 + n]).wait_recv()

    def settle(a, src, place):
        landed(a, src, place)
        multiply(a, src, False)

    half_way = Q // 2
    forward(*items[0], 0, Q)
    forward(*items[1], 0, Q)
    received(xs.at[pl.ds(0, len(peers) * CAP), :], ts.at[1])
    for a in (0, 1):
        multiply(a, f, True)
    for n in range(2, 6):
        forward(*items[n], 0, half_way)
        settle(*items[n - 2])
        forward(*items[n], half_way, Q)
        if n == 3:
            forward(2, near, 0, 0, NEAR)
    settle(*items[4])

    @pl.when(inner == 0)
    def _():
        z_send(2, 2, 1)
        z_send(2, 1, 1)

    settle(*items[5])
    activate()
    partial_out(f, 0, 0)
    partial_out(f, 0, 1)
    partial_out(near, 1, g)
    landed(2, near, 0)
    partial_out(near, 1, 1 - g)
    mix_own(0)
    mix_own(1)
    mix_near(g)
    forward(2, far_out, 1, 0, 1)
    mix_near(1 - g)
    forward(2, far_out, 1, 1, OUT)
    partial_out(far_out, 2, g)

    def forward_in(begin, end):
        forward(2, far_in, 2, begin, end)

    @pl.when(inner == 0)
    def _():
        forward_in(0, FINE)
        landed(2, far_out, 1)
        partial_out(far_out, 2, 1 - g)
        forward_in(FINE, ALL)
        share(0, g)
        share(0, 1 - g)
        partial_out(far_in, 3, g)
        landed_in(0, 1, 2)
        partial_out(far_in, 3, 1 - g)
        share(1, g)
        share(1, 1 - g)

    @pl.when(inner == 1)
    def _():
        landed(2, far_out, 1)
        partial_out(far_out, 2, 1 - g)
        forward_in(0, FINE)
        partial_out(far_in, 3, g, 0)
        forward_in(FINE, FINE + FINE // 2)
        landed_in(0)
        partial_out(far_in, 3, 1 - g, 0)
        forward_in(FINE + FINE // 2, ALL - 1)
        received(shared.at[0], mr.at[2])
        join(0, g)
        join(0, 1 - g)
        forward_in(ALL - 1, ALL)
        partial_out(far_in, 3, g, 1)
        received(shared.at[1], mr.at[3])
        join(1, g, 0)
        join(1, 1 - g, 0)
        cut = (ALL - FINE - 1) * C // FINE // 128 * 128
        landed_in(1)
        partial_early(1 - g, cut)
        landed_in(2)
        partial_late(1 - g, cut)
        join(1, g, 1)
        join(1, 1 - g, 1)

    sent(xs.at[pl.ds(0, len(peers) * CAP), :], ts.at[0])
    sent(sendw, zs.at[0])
    sent(sendt, zs.at[1])
    for a in range(3):
        sent(sendw.at[a] if a < 2 else sendt, ys.at[a])
    sent(pbf.at[pl.ds(0, len(peers) * CAP), :], ps.at[0])
    received(mrecv.at[0], mr.at[0])
    received(mrecv.at[1], mr.at[1])
    for n in range(3):
        sent(msend.at[:, pl.ds(0, R)], ms.at[n])


def deliver_kernel(gw, uw, dw, mown, mrecv, go, uo, do, mo, total, sems):
    copies = [pltpu.make_async_copy(a, b, sems.at[n]) for n, (a, b) in enumerate(((gw, go), (uw, uo), (dw, do)))]
    for copy in copies:
        copy.start()
    value = mown[...]
    for n in range(mrecv.shape[0]):
        value = value + mrecv[n].astype(jnp.float32)
    total[...] = value.astype(jnp.bfloat16)
    last = pltpu.make_async_copy(total, mo, sems.at[len(copies)])
    last.start()
    for copy in copies + [last]:
        copy.wait()


def exchange(F, T, gate, up, down, gain, tokens, routes, weight):
    span = -(-tokens.shape[0] // 128) * 128
    R, FF = gate.shape
    C, D, H = FF // F, F * R, R // 2
    Q, NEAR, OUT, FINE = 4, 1, 2, C // 128
    tok, S = tokens.shape[0], EXPERTS * CAP
    bf, f32 = jnp.bfloat16, jnp.float32
    any_spec, vm = pl.BlockSpec(memory_space=pl.ANY), pl.BlockSpec(memory_space=pltpu.VMEM)
    dma = pltpu.SemaphoreType.DMA
    held = pl.pallas_call(
        functools.partial(exchange_kernel, F, T, R, C, Q, NEAR, OUT, FINE),
        name="exchange",
        out_shape=(pltpu.VMEM((D, C), bf), pltpu.VMEM((D, C), bf), pltpu.VMEM((C, D), bf),
                   pltpu.VMEM((tok, R), f32), pltpu.VMEM((2, tok, R), bf)),
        in_specs=[any_spec] * 7,
        out_specs=(vm,) * 5,
        scratch_shapes=[
            pltpu.VMEM((1, R), f32), pltpu.VMEM((tok, D), bf), pltpu.VMEM((routes.shape[1], tok), jnp.int32),
            pltpu.VMEM((routes.shape[1], tok), f32), pltpu.VMEM((128, span), f32), pltpu.VMEM((span, 128), f32), pltpu.VMEM((R, 128), f32),
            pltpu.VMEM((3, H, C), f32), pltpu.VMEM((3, C, H), f32),
            pltpu.VMEM((2, F - 1, H, C), bf), pltpu.VMEM((F - 1, C, H), bf),
            pltpu.VMEM((tok, D), bf), pltpu.VMEM((S, D), bf), pltpu.VMEM((tok, S), bf), pltpu.VMEM((tok, S), bf),
            pltpu.VMEM((S, H // 2), f32), pltpu.VMEM((S, D), bf),
            pltpu.VMEM((S, C), f32), pltpu.VMEM((S, C), f32), pltpu.VMEM((S, C), bf),
            pltpu.VMEM((S, D), bf), pltpu.VMEM((S, D), bf), pltpu.VMEM((tok, D), bf), pltpu.VMEM((2, tok, R), bf),
            dma((2,)), dma((2, F - 1, Q)), dma((NEAR + OUT + 2 * FINE,)), dma((3,)), dma((2, F - 1)), dma((5,)), dma((2,)),
            dma((1,)), dma((5, 2)), dma((3,)), dma((4,)), dma((6,)),
        ],
        compiler_params=pltpu.CompilerParams(collective_id=0, has_side_effects=True, vmem_limit_bytes=42 * 1024 * 1024),
    )(gate, up, down, gain[None, :], tokens, routes.T, weight.T)
    return pl.pallas_call(
        deliver_kernel,
        name="deliver",
        out_shape=(jax.ShapeDtypeStruct((D, C), bf), jax.ShapeDtypeStruct((D, C), bf),
                   jax.ShapeDtypeStruct((C, D), bf), jax.ShapeDtypeStruct((tok, R), bf)),
        in_specs=[vm] * 5,
        out_specs=(pl.BlockSpec(memory_space=pltpu.HBM),) * 4,
        scratch_shapes=[pltpu.VMEM((tok, R), bf), dma((4,))],
        compiler_params=pltpu.CompilerParams(vmem_limit_bytes=4 * 1024 * 1024),
    )(*[pltpu.with_memory_space_constraint(x, pltpu.VMEM) for x in held])


def fits(grp_count, fs_count, pieces, gate_train):
    rows, wide = gate_train.shape[1:]
    return (grp_count == 2 and fs_count == pieces and fs_count == 4
            and wide % (fs_count * 128) == 0 and rows % 256 == 0)


def shards(tokens, routes, route_weight, norm_gain, gate_train, up_train, down_train):
    fs_count = lax.axis_size("fs")
    pieces = min(fs_count, 32)
    copies = fs_count // pieces
    if fits(lax.axis_size("grp"), fs_count, pieces, gate_train):
        gate_new, up_new, down_new, mixed = exchange(
            fs_count, lax.axis_size("tp"), gate_train[0], up_train[0], down_train[0],
            norm_gain, tokens, routes, route_weight,
        )
        return (gate_new[None], up_new[None], down_new[None], mixed)
    gain_column = norm_gain[:, None]
    gate_low = (gate_train[0] * gain_column).astype(jnp.bfloat16)
    up_low = (up_train[0] * gain_column).astype(jnp.bfloat16)
    down_low = down_train[0].astype(jnp.bfloat16)
    gate_wide = jnp.tile(gate_low, (1, copies))
    up_wide = jnp.tile(up_low, (1, copies))
    down_wide = jnp.tile(down_low, (copies, 1))
    gate_new, up_new = (
        lax.all_to_all(gate_wide, "fs", split_axis=1, concat_axis=0, tiled=True),
        lax.all_to_all(up_wide, "fs", split_axis=1, concat_axis=0, tiled=True),
    )
    down_new = lax.all_to_all(down_wide, "fs", split_axis=0, concat_axis=1, tiled=True)
    tok_float = tokens.astype(jnp.float32)
    normed = (
        tok_float * lax.rsqrt(jnp.mean(tok_float * tok_float, axis=-1, keepdims=True) + 1e-06)
    ).astype(jnp.bfloat16)
    chosen = routes.reshape(-1)
    chosen_hot = (chosen[:, None] == jnp.arange(EXPERTS, dtype=jnp.int32)[None, :]).astype(
        jnp.int32
    )
    before = jnp.cumsum(chosen_hot, axis=0) - chosen_hot
    slot_rank = jnp.sum(before * chosen_hot, axis=1)
    slot_index = (chosen * CAP + slot_rank).reshape(routes.shape)
    slot_range = jnp.arange(EXPERTS * CAP, dtype=jnp.int32)
    select_rows = jnp.any(slot_range[:, None, None] == slot_index[None, :, :], axis=-1).astype(
        jnp.bfloat16
    )
    outgoing = jnp.dot(select_rows, normed, preferred_element_type=jnp.float32).astype(jnp.bfloat16)
    outgoing = outgoing.reshape(EXPERTS, CAP, normed.shape[1])
    arrived = lax.all_to_all(outgoing, "tp", split_axis=0, concat_axis=0, tiled=True).reshape(
        EXPERTS * CAP, normed.shape[1]
    )
    slot_count = EXPERTS * CAP // copies
    copy_index = lax.axis_index("fs") // pieces
    my_rows = lax.dynamic_slice_in_dim(arrived, copy_index * slot_count, slot_count, 0)
    gated = jnp.dot(my_rows, gate_new, preferred_element_type=jnp.float32)
    lifted = jnp.dot(my_rows, up_new, preferred_element_type=jnp.float32)
    hidden = (jax.nn.silu(gated) * lifted).astype(jnp.bfloat16)
    partial_out = jnp.dot(hidden, down_new, preferred_element_type=jnp.float32)
    placed = jnp.zeros((EXPERTS * CAP, partial_out.shape[1]), jnp.float32)
    placed = lax.dynamic_update_slice_in_dim(placed, partial_out, copy_index * slot_count, 0)
    expert_out = lax.psum_scatter(placed, "fs", scatter_dimension=1, tiled=True).astype(
        jnp.bfloat16
    )
    returned = lax.all_to_all(
        expert_out.reshape(EXPERTS, CAP, expert_out.shape[1]),
        "tp",
        split_axis=0,
        concat_axis=0,
        tiled=True,
    )
    returned = returned.reshape(EXPERTS * CAP, expert_out.shape[1]).astype(jnp.float32)
    blend_weight = jnp.sum(
        jnp.where(
            slot_range[None, None, :] == slot_index[:, :, None], route_weight[:, :, None], 0.0
        ),
        axis=1,
    )
    mixed = jnp.dot(
        blend_weight, returned, precision=lax.Precision.HIGHEST, preferred_element_type=jnp.float32
    )
    return (gate_new[None], up_new[None], down_new[None], mixed.astype(jnp.bfloat16))


def solution(mesh):
    in_specs = (
        P(("grp", "tp"), None),
        P(("grp", "tp"), None),
        P(("grp", "tp"), None),
        P("fs"),
        P("tp", "fs", None),
        P("tp", "fs", None),
        P("tp", None, "fs"),
    )
    out_specs = (
        P(("grp", "tp"), None, "fs"),
        P(("grp", "tp"), None, "fs"),
        P(("grp", "tp"), "fs", None),
        P(("grp", "tp"), "fs"),
    )
    return jax.shard_map(shards, mesh=mesh, in_specs=in_specs, out_specs=out_specs, check_vma=False)
```
